256 devices in a mesh: sp: 64 (over z, x, core), tp: 4 (over y).
Axes of the slice: x: 4, y: 4, z: 8, core: 2. Of those that a mesh axis runs over, the one named last changes fastest.
Arguments:
- residual: bfloat16 [16384, 2048], P('sp', 'tp'), may hold values from -48 to 48
- queries: bfloat16 [16384, 1024], P('sp', 'tp'), may hold values from -6 to 6
- key_rows: bfloat16 [16384, 512], P('sp', 'tp'), may hold values from -6 to 6
- value_rows: bfloat16 [16384, 512], P('sp', 'tp'), may hold values from -6 to 6
- break_shift: bfloat16 [4, 16384], P('tp', 'sp'), may hold values from -20 to 0
- head_gain: float32 [1024], P('tp'), may hold values from 0.1 to 1.9
- out_weight: bfloat16 [1024, 2048], P('tp'), may hold values from -0.1875 to 0.1875
- mlp_gain: float32 [2048], replicated, may hold values from 0.1 to 1.9
- up_weight: bfloat16 [2048, 8192], P('sp', 'tp'), may hold values from -0.125 to 0.125
- down_weight: bfloat16 [8192, 2048], P('tp', 'sp'), may hold values from -0.0625 to 0.0625
Outputs:
- layer_out: bfloat16 [16384, 2048], P('sp', 'tp')
The draws below stay inside these ranges and needn't reach their ends.
All inputs are finite; a program needn't handle non-finite values.
Results may differ from the reference program's by a relative error of at most 0.013.
Values may be sent and summed in bfloat16 or wider, within the bound.
A program may use at most 128 MiB of HBM per device.

```python
import math
import jax
import jax.numpy as jnp
from jax import lax

D = 2048
HEADS = 8
KEY_VALUE_HEADS = 4
HEAD_DIM = 128
FF = 8192
TOK_DEV = 256
TOKEN_POSITIONS = 16384
KEY_BLOCK = 2048


def draw_residual(key, part):
    noise_key, row_key = jax.random.split(jax.random.fold_in(key, 11), 2)
    column_scale = jnp.exp(math.log(3.0) * jnp.arange(D, dtype=jnp.float32) / D)
    entries = jax.random.truncated_normal(noise_key, -6.0, 6.0, (TOKEN_POSITIONS, D), jnp.float32)
    row_scale = jnp.exp(jax.random.uniform(row_key, (TOKEN_POSITIONS, 1), jnp.float32, 0.0, math.log(10.0)))
    return (entries * row_scale * column_scale / 4.0).astype(jnp.bfloat16)


def draw_break_shift(key, part):
    variety_random_key, frequency_random_key, quick_random_key, block_random_key, spike_random_key, depth_random_key = jax.random.split(jax.random.fold_in(key, 29), 6)
    ranking = jax.random.permutation(variety_random_key, KEY_VALUE_HEADS)
    slow_heads = (ranking < KEY_VALUE_HEADS // 2).astype(jnp.float32)[:, None]
    slow_level = -math.log(float(TOKEN_POSITIONS)) + jax.random.uniform(frequency_random_key, (KEY_VALUE_HEADS, 1), jnp.float32, math.log(0.5), 0.0)
    fast_level = jax.random.uniform(quick_random_key, (KEY_VALUE_HEADS, 1), jnp.float32, -4.5, -3.5)
    baseline_level = slow_heads * slow_level + (1.0 - slow_heads) * fast_level
    block_raise = jax.random.uniform(block_random_key, (KEY_VALUE_HEADS, TOKEN_POSITIONS // TOK_DEV), jnp.float32, 0.0, math.log(4.0))
    block_raise = jnp.repeat(block_raise, TOK_DEV, axis=1)
    spike_locations = jax.random.randint(spike_random_key, (3,), 0, TOKEN_POSITIONS)
    spike_flag = jnp.any(jnp.arange(TOKEN_POSITIONS, dtype=jnp.int32)[None, :] == spike_locations[:, None], axis=0)
    spike_level = jax.random.uniform(depth_random_key, (KEY_VALUE_HEADS, TOKEN_POSITIONS), jnp.float32, -1.6, -0.6)
    return jnp.where(spike_flag[None, :], spike_level, baseline_level + block_raise).astype(jnp.bfloat16)


def block_levels(own_key, dims, shards, smallest, high):
    loudness, own = 1.0, jax.random.fold_in(own_key, 6)
    for dim, blocks in shards:
        steps = jnp.exp(jax.random.uniform(jax.random.fold_in(own, dim), (blocks,), jnp.float32, smallest / len(shards), high / len(shards)))
        loudness = loudness * jnp.repeat(steps, dims[dim] // blocks).reshape([-1 if axis == dim else 1 for axis in range(len(dims))])
    return loudness


def noise(stream_key, dims, deviation, bound, pieces=(), kind=jnp.bfloat16):
    values = deviation * jax.random.normal(stream_key, dims, jnp.float32)
    if pieces:
        values = values * block_levels(stream_key, dims, pieces, -0.22, 0.18)
    return jnp.clip(values, -bound, bound).astype(kind)


def setup_inputs(seed: int = 0) -> dict:
    key_of = jax.random.split(jax.random.key(seed), 11)
    return {
        "residual": draw_residual(jax.random.fold_in(key_of[10], 71), 0),
        "queries": noise(key_of[1], (TOKEN_POSITIONS, HEADS * HEAD_DIM), 1.0, 6.0, ((0, 64), (1, 4))),
        "key_rows": noise(key_of[2], (TOKEN_POSITIONS, KEY_VALUE_HEADS * HEAD_DIM), 1.0, 6.0, ((0, 64), (1, 4))),
        "value_rows": noise(key_of[3], (TOKEN_POSITIONS, KEY_VALUE_HEADS * HEAD_DIM), 1.0, 6.0, ((0, 64), (1, 4))),
        "break_shift": draw_break_shift(jax.random.fold_in(key_of[10], 71), 0),
        "head_gain": jnp.clip(1.0 + 0.18 * jax.random.normal(key_of[5], (HEADS * HEAD_DIM,), jnp.float32), 0.1, 1.9),
        "out_weight": noise(key_of[6], (HEADS * HEAD_DIM, D), (HEADS * HEAD_DIM) ** -0.5, 0.1875, ((0, 4),)),
        "mlp_gain": jnp.clip(1.0 + 0.18 * jax.random.normal(key_of[7], (D,), jnp.float32), 0.1, 1.9),
        "up_weight": noise(key_of[8], (D, FF), D ** -0.5, 0.125, ((0, 64), (1, 4))),
        "down_weight": noise(key_of[9], (FF, D), FF ** -0.5, 0.0625, ((0, 4), (1, 64))),
    }


eps = 1e-06

def reference(residual, queries, key_rows, value_rows, break_shift, head_gain, out_weight, mlp_gain, up_weight, down_weight):
    group_size = HEADS // KEY_VALUE_HEADS
    block_total = TOKEN_POSITIONS // KEY_BLOCK
    score_scale = HEAD_DIM ** (-0.5)
    query_grid = queries.astype(jnp.float32).reshape(TOKEN_POSITIONS, KEY_VALUE_HEADS, group_size, HEAD_DIM)
    key_grid = key_rows.astype(jnp.float32).reshape(TOKEN_POSITIONS, KEY_VALUE_HEADS, HEAD_DIM)
    value_grid = value_rows.astype(jnp.float32).reshape(TOKEN_POSITIONS, KEY_VALUE_HEADS, HEAD_DIM)
    shift_grid = break_shift.astype(jnp.float32)

    def query_span(span_index):
        first_pos = span_index * KEY_BLOCK
        query_block = lax.dynamic_slice_in_dim(query_grid, first_pos, KEY_BLOCK, 0)
        query_pos = first_pos + lax.iota(jnp.int32, KEY_BLOCK)

        def one_block(turn_index, state_pair):
            running, broken_after = state_pair
            offset = (span_index - turn_index) * KEY_BLOCK
            key_block_rows = lax.dynamic_slice_in_dim(key_grid, offset, KEY_BLOCK, 0)
            value_block_rows = lax.dynamic_slice_in_dim(value_grid, offset, KEY_BLOCK, 0)
            shift_block = lax.dynamic_slice_in_dim(shift_grid, offset, KEY_BLOCK, 1)
            scores = jnp.einsum('qgjd,kgd->gjqk', query_block, key_block_rows) * score_scale + shift_block[:, None, None, :]
            key_pos = offset + lax.iota(jnp.int32, KEY_BLOCK)
            visible = key_pos[None, None, None, :] < query_pos[None, None, :, None]
            broken = jnp.where(visible, jax.nn.log_sigmoid(-scores), 0.0)
            later = lax.cumsum(broken, axis=3, reverse=True) - broken + broken_after[:, :, :, None]
            weights = jnp.where(visible, jnp.exp(jax.nn.log_sigmoid(scores) + later), 0.0).astype(jnp.bfloat16)
            weights = lax.optimization_barrier(weights).astype(jnp.float32)
            running = running + jnp.einsum('gjqk,kgd->gjqd', weights, value_block_rows)
            return (running, broken_after + lax.optimization_barrier(jnp.sum(broken, axis=3)))
        start_pair = (jnp.zeros((KEY_VALUE_HEADS, group_size, KEY_BLOCK, HEAD_DIM), jnp.float32), jnp.zeros((KEY_VALUE_HEADS, group_size, KEY_BLOCK), jnp.float32))
        running, broken_after = lax.fori_loop(0, span_index + 1, one_block, start_pair)
        return running.transpose(2, 0, 1, 3).reshape(KEY_BLOCK, HEADS, HEAD_DIM)
    mixed = lax.map(query_span, jnp.arange(block_total, dtype=jnp.int32)).reshape(TOKEN_POSITIONS, HEADS, HEAD_DIM)
    power = lax.optimization_barrier(jnp.mean(mixed * mixed, axis=2, keepdims=True))
    attended = (mixed * lax.rsqrt(power + eps) * head_gain.astype(jnp.float32).reshape(HEADS, HEAD_DIM)).astype(jnp.bfloat16)
    attended = attended.reshape(TOKEN_POSITIONS, HEADS * HEAD_DIM)
    hidden_state = (residual.astype(jnp.float32) + jnp.dot(attended, out_weight, preferred_element_type=jnp.float32)).astype(jnp.bfloat16)
    widened = hidden_state.astype(jnp.float32)
    mlp_in = (widened * lax.rsqrt(lax.optimization_barrier(jnp.mean(widened * widened, axis=1, keepdims=True)) + eps) * mlp_gain.astype(jnp.float32)).astype(jnp.bfloat16)
    activated = jnp.square(jax.nn.relu(jnp.dot(mlp_in, up_weight, preferred_element_type=jnp.float32))).astype(jnp.bfloat16)
    return (widened + jnp.dot(activated, down_weight, preferred_element_type=jnp.float32)).astype(jnp.bfloat16)
```

```python
import functools
import math

import jax
import jax.numpy as jnp
from jax import lax
from jax.experimental import pallas as pl
from jax.experimental.pallas import tpu as pltpu
from jax.sharding import PartitionSpec as P

MESH = pl.DeviceIdType.MESH
HEAD_DIM = 128
EPS = 1e-06
LOG2E = 1.4426950408889634
SCALE2 = LOG2E / math.sqrt(HEAD_DIM)
NT = (((1,), (1,)), ((), ()))
F32 = jnp.float32
BF16 = jnp.bfloat16
KV_SUBS = 2
W_SUBS = 4
STEPS = 16


def ring_one_position(x, z):
    return 4 * z + lax.rem(x + z, 4)


def ring_one_chip(p):
    row = lax.div(p, 4)
    return 4 * row + lax.rem(p + 3 * row, 4)


def ring_two_position(x, z):
    d = lax.rem(z + 5 * x, 8)
    return 4 * x + d + 12 * lax.div(d, 4)


def ring_two_chip(p):
    seg = lax.div(p, 4)
    return 4 * lax.rem(3 * seg + lax.rem(p, 4), 8) + lax.rem(seg, 4)


def kernel(
    res_ref, q_ref, k_ref, v_ref, gain_ref, ow_ref, mg_ref, up_ref, dn_ref, out_ref,
    kg, vg, upg, dng, owg, resg, attg, qs, acc, carry, hid, mi, act, rs_out, rs_in, own_part,
    kv_recv, w_recv, kv_send, w_send, kv_pair_send, kv_pair_recv, w_pair_send, w_pair_recv,
    local_sem, ow_send, ow_recv, ow_pair_send, ow_pair_recv, res_send, res_recv,
    att_send, att_recv, rs_send, rs_recv,
):
    sp = lax.axis_index("sp")
    tp = lax.axis_index("tp")
    core = lax.rem(sp, 2)
    chip = lax.div(sp, 2)
    x, z = lax.rem(chip, 4), lax.div(chip, 4)
    partner = (sp + 1 - 2 * core, tp)
    p1, p2 = ring_one_position(x, z), ring_two_position(x, z)

    def on_ring(ring, p):
        return 2 * (ring_one_chip(p) if ring == 0 else ring_two_chip(p)) + core

    here = (p1, p2)
    nxt = [(on_ring(r, lax.rem(here[r] + 1, 32)), tp) for r in (0, 1)]
    prv = [(on_ring(r, lax.rem(here[r] + 31, 32)), tp) for r in (0, 1)]
    target = (nxt[0], prv[0], nxt[1], prv[1])
    peers = [(sp, lax.rem(tp + d, 4)) for d in (1, 2, 3)]
    everyone = [nxt[0], prv[0], nxt[1], prv[1], partner] + peers

    barrier = pltpu.get_barrier_semaphore()
    for device in everyone:
        pl.semaphore_signal(barrier, inc=1, device_id=device, device_id_type=MESH)
    pl.semaphore_wait(barrier, len(everyone))

    def remote(src, dst, send_sem, recv_sem, device):
        return pltpu.make_async_remote_copy(
            src_ref=src, dst_ref=dst, send_sem=send_sem, recv_sem=recv_sem,
            device_id=device, device_id_type=MESH,
        )

    def waits(ref, sem):
        pltpu.make_async_copy(ref, ref, sem).wait()

    def kv_slot(ring, origin, sub):
        return (kg if ring == 0 else vg).at[origin * KV_SUBS + sub]

    def w_slot(ring, origin, sub):
        rows = pl.ds(pl.multiple_of(origin * 32, 32), 32)
        return (upg if ring == 0 else dng).at[sub, rows, :]

    for sub in range(KV_SUBS):
        for j in range(4):
            ring = j // 2
            src = (k_ref if ring == 0 else v_ref).at[sub]
            remote(src, kv_slot(ring, sp, sub), kv_send.at[j], kv_recv.at[j, sub], target[j]).start()
    for sub in range(W_SUBS):
        for j in range(4):
            ring = j // 2
            src = (up_ref if ring == 0 else dn_ref).at[:, pl.ds(sub * 512, 512)]
            remote(src, w_slot(ring, sp, sub), w_send.at[j], w_recv.at[j, sub], target[j]).start()
    half = pl.ds(pl.multiple_of(core * 1024, 1024), 1024)
    for d in (1, 2, 3):
        remote(res_ref, resg.at[tp], res_send.at[d - 1], res_recv.at[d - 1], peers[d - 1]).start()
    for d in (1, 2, 3):
        remote(
            ow_ref.at[:, half], owg.at[tp, core], ow_send.at[d - 1], ow_recv.at[d - 1], peers[d - 1]
        ).start()
    locals_ = []

    def keep(src, dst):
        copy = pltpu.make_async_copy(src, dst, local_sem.at[len(locals_)])
        copy.start()
        locals_.append(copy)

    for ring in (0, 1):
        for sub in range(KV_SUBS):
            src = (k_ref if ring == 0 else v_ref).at[sub]
            remote(
                src, kv_slot(ring, sp, sub), kv_pair_send.at[ring], kv_pair_recv.at[ring], partner
            ).start()
            keep(src, kv_slot(ring, sp, sub))
        for sub in range(W_SUBS):
            src = (up_ref if ring == 0 else dn_ref).at[:, pl.ds(sub * 512, 512)]
            remote(
                src, w_slot(ring, sp, sub), w_pair_send.at[ring], w_pair_recv.at[ring], partner
            ).start()
            keep(src, w_slot(ring, sp, sub))
    for c in range(2):
        keep(ow_ref.at[:, pl.ds(c * 1024, 1024)], owg.at[tp, c])
    keep(res_ref, resg.at[tp])
    qs[0:256, :] = q_ref[:, 0:128]
    qs[256:512, :] = q_ref[:, 128:256]

    def ring_step(n, subs, slot, send, recv, pair_send, pair_recv):
        s = lax.div(n, subs) + 1
        sub = lax.rem(n, subs)
        for j in range(4):
            ring, back = j // 2, j % 2
            last = STEPS - back
            p = here[ring]
            origin = on_ring(ring, lax.rem(p + s, 32) if back else lax.rem(p + 32 - s, 32))
            block = slot(ring, origin, sub)

            @pl.when(s <= last)
            def _():
                remote(block, block, send.at[j], recv.at[j, n], target[j]).wait_recv()

            @pl.when(s < last)
            def _():
                remote(block, block, send.at[j], recv.at[j, n + subs], target[j]).start()

            @pl.when(s <= last)
            def _():
                remote(block, block, pair_send.at[ring], pair_recv.at[ring], partner).start()

    def kv_step(n):
        ring_step(n, KV_SUBS, kv_slot, kv_send, kv_recv, kv_pair_send, kv_pair_recv)

    def w_step(n):
        ring_step(n, W_SUBS, w_slot, w_send, w_recv, w_pair_send, w_pair_recv)

    kv_total, w_total = STEPS * KV_SUBS, STEPS * W_SUBS

    def gather_keys(n, _):
        kv_step(n)
        w_step(n)
        return 0

    lax.fori_loop(0, kv_total, gather_keys, 0)
    for ring in (0, 1):
        buf = kg if ring == 0 else vg
        waits(buf.at[0:64], kv_pair_recv.at[ring])
    for copy in locals_:
        copy.wait()

    row = lax.broadcasted_iota(jnp.int32, (256, 256), 0)
    col = lax.broadcasted_iota(jnp.int32, (256, 256), 1)
    later_keys = (row > col).astype(BF16)
    acc[...] = jnp.zeros_like(acc)
    carry[...] = jnp.zeros_like(carry)

    def attend(block, diagonal):
        both = pl.ds(pl.multiple_of(block * 2, 2), 2)
        keys = kg[both, 0:128, :].reshape(256, 128)
        values = vg[both, :, :].reshape(256, 128)
        shift = kg[both, 128:144, :].astype(F32) * LOG2E
        shift = jnp.concatenate([shift[0, 0:1, :], shift[1, 0:1, :]], axis=1)
        t = lax.dot_general(qs[...], keys, NT, preferred_element_type=F32) * SCALE2 + shift
        soft = jnp.maximum(t, jnp.log2(1.0 + jnp.exp2(jnp.minimum(t, 126.0))))
        broken = soft
        if diagonal:
            q_pos = lax.rem(lax.broadcasted_iota(jnp.int32, (512, 256), 0), 256)
            visible = lax.broadcasted_iota(jnp.int32, (512, 256), 1) < q_pos
            broken = jnp.where(visible, soft, 0.0)
        later = jnp.dot(broken.astype(BF16), later_keys, preferred_element_type=F32)
        after = carry[...]
        weights = jnp.exp2((t - soft) - (later + after))
        if diagonal:
            weights = jnp.where(visible, weights, 0.0)
        acc[...] += jnp.dot(weights.astype(BF16), values, preferred_element_type=F32)
        carry[...] = after + (later[:, 0:1] + broken[:, 0:1])

    attend(sp, True)

    def beside_weights(n, _):
        w_step(n)
        block = sp - 1 - (n - kv_total)

        @pl.when(block >= 0)
        def _():
            attend(jnp.maximum(block, 0), False)

        return 0

    lax.fori_loop(kv_total, w_total, beside_weights, 0)
    for d in (1, 2, 3):
        source = lax.rem(tp + 4 - d, 4)
        block = owg.at[source, core]
        remote(block, block, ow_send.at[d - 1], ow_recv.at[d - 1], partner).wait_recv()
        remote(block, block, ow_pair_send, ow_pair_recv, partner).start()
    done = w_total - kv_total
    lax.fori_loop(
        done, jnp.maximum(sp, done), lambda n, _: (attend(sp - 1 - n, False), 0)[1], 0
    )

    for h in range(2):
        mixed = acc[pl.ds(h * 256, 256), :]
        power = jnp.mean(mixed * mixed, axis=1, keepdims=True)
        lanes = slice(h * 128, h * 128 + 128)
        attg[tp, :, lanes] = (mixed * lax.rsqrt(power + EPS) * gain_ref[0:1, lanes]).astype(BF16)
    for d in (2, 1, 3):
        remote(
            attg.at[tp], attg.at[tp], att_send.at[d - 1], att_recv.at[d - 1], peers[d - 1]
        ).start()
    waits(owg.at[0:3, 0], ow_pair_recv)
    for d in (1, 2, 3):
        block = resg.at[tp]
        remote(block, block, res_send.at[d - 1], res_recv.at[d - 1], peers[d - 1]).wait_recv()
    for d in (1, 2, 3):
        block = attg.at[tp]
        remote(block, block, att_send.at[d - 1], att_recv.at[d - 1], peers[d - 1]).wait_recv()

    squares = jnp.zeros((256, 1), F32)
    for b in range(4):
        total = resg[b].astype(F32)
        for g in range(4):
            weight = owg[g, b // 2, :, (b % 2) * 512 : (b % 2) * 512 + 512]
            total = total + jnp.dot(attg[g], weight, preferred_element_type=F32)
        hidden = total.astype(BF16)
        hid[b] = hidden
        wide = hidden.astype(F32)
        squares = squares + jnp.sum(wide * wide, axis=1, keepdims=True)
    inverse = lax.rsqrt(squares / 2048.0 + EPS)
    for b in range(4):
        mi[:, b * 512 : b * 512 + 512] = (hid[b].astype(F32) * inverse * mg_ref[b]).astype(BF16)

    waits(upg.at[0:2], w_pair_recv.at[0])
    waits(dng.at[0:2], w_pair_recv.at[1])
    for b in range(4):
        lifted = jnp.dot(mi[...], upg[b], preferred_element_type=F32)
        lifted = jnp.maximum(lifted, 0.0)
        act[b] = (lifted * lifted).astype(BF16)

    def down(owner):
        rows = pl.ds(pl.multiple_of(owner * 512, 512), 512)
        total = jnp.zeros((256, 512), F32)
        for b in range(4):
            total = total + lax.dot_general(
                act[b], dng[b, rows, :], NT, preferred_element_type=F32
            )
        return total

    for d in (2, 1, 3):
        rs_out[d - 1] = down(lax.rem(tp + d, 4)).astype(BF16)
        remote(
            rs_out.at[d - 1], rs_in.at[d - 1], rs_send.at[d - 1], rs_recv.at[d - 1], peers[d - 1]
        ).start()
    own_part[...] = down(tp) + hid[tp].astype(F32)
    for d in (1, 3, 2):
        remote(
            rs_out.at[d - 1], rs_in.at[d - 1], rs_send.at[d - 1], rs_recv.at[d - 1], peers[d - 1]
        ).wait_recv()
    out_ref[...] = (
        own_part[...] + rs_in[0].astype(F32) + rs_in[1].astype(F32) + rs_in[2].astype(F32)
    ).astype(BF16)

    for j in range(4):
        ring, back = j // 2, j % 2
        waits((kg if ring == 0 else vg).at[0 : 32 - 2 * back], kv_send.at[j])
        waits((upg if ring == 0 else dng).at[0, 0 : 2048 - 128 * back, :], w_send.at[j])
    for ring in (0, 1):
        waits((kg if ring == 0 else vg).at[0:64], kv_pair_send.at[ring])
        waits((upg if ring == 0 else dng).at[0:2], w_pair_send.at[ring])
    waits(owg.at[0:3, 0], ow_pair_send)
    for d in (1, 2, 3):
        waits(res_ref, res_send.at[d - 1])
        waits(owg.at[0, 0], ow_send.at[d - 1])
        waits(attg.at[0], att_send.at[d - 1])
        waits(rs_out.at[d - 1], rs_send.at[d - 1])


def body(
    residual, queries, key_rows, value_rows, break_shift, head_gain, out_weight, mlp_gain,
    up_weight, down_weight,
):
    shift = jnp.pad(break_shift.reshape(2, 1, 128), ((0, 0), (0, 15), (0, 0)))
    keys = jnp.concatenate([key_rows.reshape(2, 128, 128), shift], axis=1)
    values = value_rows.reshape(2, 128, 128)
    vmem = pltpu.VMEM
    dma = pltpu.SemaphoreType.DMA
    return pl.pallas_call(
        kernel,
        out_shape=jax.ShapeDtypeStruct((256, 512), BF16),
        in_specs=[pl.BlockSpec(memory_space=vmem)] * 9,
        out_specs=pl.BlockSpec(memory_space=vmem),
        scratch_shapes=[
            vmem((128, 144, 128), BF16),
            vmem((128, 128, 128), BF16),
            vmem((4, 2048, 512), BF16),
            vmem((4, 2048, 512), BF16),
            vmem((4, 2, 256, 1024), BF16),
            vmem((4, 256, 512), BF16),
            vmem((4, 256, 256), BF16),
            vmem((512, 128), BF16),
            vmem((512, 128), F32),
            vmem((512, 1), F32),
            vmem((4, 256, 512), BF16),
            vmem((256, 2048), BF16),
            vmem((4, 256, 512), BF16),
            vmem((3, 256, 512), BF16),
            vmem((3, 256, 512), BF16),
            vmem((256, 512), F32),
            dma((4, STEPS * KV_SUBS)),
            dma((4, STEPS * W_SUBS)),
            dma((4,)),
            dma((4,)),
            dma((2,)),
            dma((2,)),
            dma((2,)),
            dma((2,)),
            dma((15,)),
            dma((3,)),
            dma((3,)),
            dma,
            dma,
            dma((3,)),
            dma((3,)),
            dma((3,)),
            dma((3,)),
            dma((3,)),
            dma((3,)),
        ],
        compiler_params=pltpu.CompilerParams(
            collective_id=0, has_side_effects=True, vmem_limit_bytes=60 * 1024 * 1024
        ),
        name="layer",
    )(
        residual, queries, keys, values, head_gain.reshape(1, 256), out_weight,
        mlp_gain.reshape(4, 1, 512), up_weight, down_weight.T,
    )


def solution(mesh):
    in_specs = (
        P("sp", "tp"),
        P("sp", "tp"),
        P("sp", "tp"),
        P("sp", "tp"),
        P("tp", "sp"),
        P("tp"),
        P("tp", None),
        P(),
        P("sp", "tp"),
        P("tp", "sp"),
    )
    return jax.shard_map(
        body, mesh=mesh, in_specs=in_specs, out_specs=P("sp", "tp"), check_vma=False
    )
```

```python
import functools
import math

import jax
import jax.numpy as jnp
from jax import lax
from jax.experimental import pallas as pl
from jax.experimental.pallas import tpu as pltpu
from jax.sharding import PartitionSpec as P

MESH = pl.DeviceIdType.MESH
HEAD_DIM = 128
EPS = 1e-06
LOG2E = 1.4426950408889634
SCALE2 = LOG2E / math.sqrt(HEAD_DIM)
NT = (((1,), (1,)), ((), ()))
F32 = jnp.float32
BF16 = jnp.bfloat16
KV_ROWS = 528
KV_PIECES = 3
KV_PIECE = KV_ROWS // KV_PIECES
UP_PIECES = 3
DOWN_PIECES = 5
X_SIZE, Z_SIZE = 4, 8


def offset_of(k, size):
    return jnp.where(lax.rem(k, 2) == 1, lax.div(k + 1, 2), lax.rem(size - lax.div(k, 2), size))


def last_step(size, direction, even):
    return size // 2 - jnp.where(even == (direction == 0), 0, 1)


def kernel(
    res_ref, q_ref, kv_ref, gain_ref, ow_ref, mg_ref, up_ref, dn_ref, out_ref,
    kvg, wg, owg, resg, attg, qg, part, total_out, part_in, total_in, acc, carry, hid, mi, act, rs_out, rs_in, own_part,
    row_recv, side_recv, kv_send, kv_pair_send, kv_pair_recv, q_send, q_recv,
    part_send, part_recv, total_send, total_recv,
    ua_recv, um_recv, da_recv, dm_recv, gather_send, pair_send, pair_recv,
    local_sem, ow_send, ow_recv, ow_pair_send, ow_pair_recv, res_send, res_recv,
    att_send, att_recv, rs_send, rs_recv,
):
    sp = lax.axis_index("sp")
    tp = lax.axis_index("tp")
    core = lax.rem(sp, 2)
    chip = lax.div(sp, 2)
    x, z = lax.rem(chip, 4), lax.div(chip, 4)
    partner = (sp + 1 - 2 * core, tp)

    def device_at(x, z):
        return 2 * (X_SIZE * z + x) + core

    x_sides = [(device_at(lax.rem(x + d, X_SIZE), z), tp) for d in (1, X_SIZE - 1)]
    z_sides = [(device_at(x, lax.rem(z + d, Z_SIZE)), tp) for d in (1, Z_SIZE - 1)]
    peers = [(sp, lax.rem(tp + d, 4)) for d in (1, 2, 3)]
    below = [(device_at(x, lax.rem(z + Z_SIZE - 2 * (i + 1), Z_SIZE)), tp) for i in range(3)]
    everyone = x_sides + z_sides + [partner] + below + peers

    barrier = pltpu.get_barrier_semaphore()
    for device in everyone:
        pl.semaphore_signal(barrier, inc=1, device_id=device, device_id_type=MESH)
    pl.semaphore_wait(barrier, len(everyone))

    def remote(src, dst, send_sem, recv_sem, device):
        return pltpu.make_async_remote_copy(
            src_ref=src, dst_ref=dst, send_sem=send_sem, recv_sem=recv_sem,
            device_id=device, device_id_type=MESH,
        )

    def waits(ref, sem):
        pltpu.make_async_copy(ref, ref, sem).wait()

    def w_slot(first):
        def slot(origin, piece):
            return wg.at[first + piece, pl.ds(pl.multiple_of(origin * 32, 32), 32), :]

        return slot

    def w_source(page):
        ref, block = (dn_ref, page) if page < 4 else (up_ref, (3, 0, 1, 2)[page - 4])
        return ref.at[:, pl.ds(block * 512, 512)]

    class Gather:
        def __init__(self, number, x_first, pieces, slot, sources, first_recv, main_recv, pair):
            self.x_first, self.pieces, self.slot, self.sources = x_first, pieces, slot, sources
            self.first_recv, self.main_recv, self.pair = first_recv, main_recv, pair
            self.first_size, self.main_size = (X_SIZE, Z_SIZE) if x_first else (Z_SIZE, X_SIZE)
            self.first_to, self.main_to = (x_sides, z_sides) if x_first else (z_sides, x_sides)
            self.sem = lambda phase, d: gather_send.at[number * 4 + phase * 2 + d]

        def origin(self, first, main):
            first_at, main_at = (x, z) if self.x_first else (z, x)
            a = lax.rem(first_at + first, self.first_size)
            b = lax.rem(main_at + main, self.main_size)
            return device_at(a, b) if self.x_first else device_at(b, a)

        def send_first(self, src, dst, d, step, piece):
            return remote(
                src, dst, self.sem(0, d), self.first_recv.at[d, step - 1, piece], self.first_to[d]
            )

        def send_main(self, src, dst, d, step, k, piece):
            return remote(
                src, dst, self.sem(1, d), self.main_recv.at[d, step - 1, k, piece], self.main_to[d]
            )

        def to_partner(self, src, dst):
            remote(src, dst, pair_send.at[self.pair], pair_recv.at[self.pair], partner).start()

        def own(self):
            for piece in range(self.pieces):
                src, dst = self.sources[piece], self.slot(sp, piece)
                for d in range(2):
                    self.send_first(src, dst, d, 1, piece).start()
            for piece in range(self.pieces):
                src, dst = self.sources[piece], self.slot(sp, piece)
                for d in range(2):
                    self.send_main(src, dst, d, 1, 0, piece).start()

        def own_near(self):
            for piece in range(self.pieces):
                src, dst = self.sources[piece], self.slot(sp, piece)
                self.to_partner(src, dst)
                keep(src, dst)

        def first_step(self, step, piece):
            for d in range(2):
                last = last_step(self.first_size, d, lax.rem(piece, 2) == 0)
                ahead = self.first_size - step if d == 0 else step
                k = jnp.minimum(2 * step, self.first_size - 1) if d == 0 else 2 * step - 1
                block = self.slot(self.origin(ahead, 0), piece)

                @pl.when(step <= last)
                def _():
                    self.send_first(block, block, d, step, piece).wait_recv()

                @pl.when(step < last)
                def _():
                    self.send_first(block, block, d, step + 1, piece).start()

                @pl.when(step <= last)
                def _():
                    for e in range(2):
                        self.send_main(block, block, e, 1, k, piece).start()
                    self.to_partner(block, block)

        def main_step(self, step, k, piece):
            for d in range(2):
                last = last_step(self.main_size, d, lax.rem(k, 2) == 0)
                ahead = self.main_size - step if d == 0 else step
                block = self.slot(self.origin(offset_of(k, self.first_size), ahead), piece)

                @pl.when(step <= last)
                def _():
                    self.send_main(block, block, d, step, k, piece).wait_recv()

                @pl.when(step < last)
                def _():
                    self.send_main(block, block, d, step + 1, k, piece).start()

                @pl.when(step <= last)
                def _():
                    self.to_partner(block, block)

        def sent(self, phase, d):
            if phase == 0:
                long = [(piece % 2 == 0) == (d == 0) for piece in range(self.pieces)]
                return sum(self.first_size // 2 - (not far) for far in long)
            return self.pieces * self.first_size * (self.main_size - 1) // 2

    locals_ = []

    def keep(src, dst):
        copy = pltpu.make_async_copy(src, dst, local_sem.at[len(locals_)])
        copy.start()
        locals_.append(copy)

    up_in = Gather(
        0, True, UP_PIECES, w_slot(5), [w_source(p) for p in (5, 6, 7)], ua_recv, um_recv, 0
    )
    down_in = Gather(
        1, False, DOWN_PIECES, w_slot(0), [w_source(p) for p in range(5)], da_recv, dm_recv, 0
    )

    row = lax.rem(z, 2)
    here = (row * X_SIZE + x) * 2 + core
    beside = (device_at(x, z + 1 - 2 * row), tp)

    def kv_slot(at_row, at_x, piece, at_core=core):
        start = pl.multiple_of(piece * KV_PIECE, KV_PIECE)
        return kvg.at[(at_row * X_SIZE + at_x) * 2 + at_core, pl.ds(start, KV_PIECE), :]

    def kv_source(piece):
        return kv_ref.at[pl.ds(pl.multiple_of(piece * KV_PIECE, KV_PIECE), KV_PIECE), :]

    def to_row(src, piece):
        return remote(src, kv_slot(row, x, piece), kv_send.at[2], row_recv.at[piece], beside)

    def to_side(src, d, step, at_row, at_x, piece):
        recv = side_recv.at[d, step - 1, at_row, piece]
        return remote(src, kv_slot(at_row, at_x, piece), kv_send.at[d], recv, x_sides[d])

    def to_core(src, at_row, at_x, piece):
        remote(src, kv_slot(at_row, at_x, piece), kv_pair_send, kv_pair_recv, partner).start()

    def send_own(piece, _):
        src = kv_source(piece)
        to_row(src, piece).start()
        for d in range(2):
            to_side(src, d, 1, row, x, piece).start()
        to_core(src, row, x, piece)
        return 0

    lax.fori_loop(0, KV_PIECES, send_own, 0)
    keep(kv_ref, kvg.at[here])
    for i in range(3):

        @pl.when(z >= 2 * (i + 1))
        def _():
            for h in range(2):
                remote(
                    q_ref.at[:, pl.ds(h * 128, 128)], qg.at[i, pl.ds(h * 256, 256), :],
                    q_send.at[i], q_recv.at[i], below[i],
                ).start()

    for h in range(2):
        keep(q_ref.at[:, pl.ds(h * 128, 128)], qg.at[3, pl.ds(h * 256, 256), :])

    def from_row(piece, _):
        at_row = 1 - row
        block = kv_slot(at_row, x, piece)
        remote(block, block, kv_send.at[2], row_recv.at[piece], beside).wait_recv()
        for d in range(2):
            to_side(block, d, 1, at_row, x, piece).start()
        to_core(block, at_row, x, piece)
        return 0

    def from_side(at_row, step, piece):
        for d in range(2):
            at_x = lax.rem(x + (X_SIZE - step if d == 0 else step), X_SIZE)
            block = kv_slot(at_row, at_x, piece)
            long = at_row == d

            def arrives():
                recv = side_recv.at[d, step - 1, at_row, piece]
                remote(block, block, kv_send.at[d], recv, x_sides[d]).wait_recv()

            if step == 1:
                arrives()

                @pl.when(long)
                def _():
                    to_side(block, d, 2, at_row, at_x, piece).start()

                to_core(block, at_row, at_x, piece)
            else:

                @pl.when(long)
                def _():
                    arrives()
                    to_core(block, at_row, at_x, piece)

    def near_side(piece, _):
        from_side(row, 1, piece)
        return 0

    def far_sides(piece, _):
        from_side(1 - row, 1, piece)
        from_side(row, 2, piece)
        return 0

    def last_side(piece, _):
        from_side(1 - row, 2, piece)
        return 0

    lax.fori_loop(0, KV_PIECES, from_row, 0)
    lax.fori_loop(0, KV_PIECES, near_side, 0)
    up_in.own()
    down_in.own()
    up_in.own_near()
    down_in.own_near()
    lax.fori_loop(0, KV_PIECES, far_sides, 0)
    lax.fori_loop(0, KV_PIECES, last_side, 0)
    half = pl.ds(pl.multiple_of(core * 1024, 1024), 1024)
    for d in (1, 2, 3):
        remote(res_ref, resg.at[tp], res_send.at[d - 1], res_recv.at[d - 1], peers[d - 1]).start()
    for d in (1, 2, 3):
        remote(
            ow_ref.at[:, half], owg.at[tp, core], ow_send.at[d - 1], ow_recv.at[d - 1], peers[d - 1]
        ).start()
    for c in range(2):
        keep(ow_ref.at[:, pl.ds(c * 1024, 1024)], owg.at[tp, c])
    keep(res_ref, resg.at[tp])
    w_first_steps = DOWN_PIECES * Z_SIZE // 2
    w_steps = w_first_steps + DOWN_PIECES * 16

    def w_step(n):
        @pl.when(n < w_first_steps)
        def _():
            step, piece = lax.div(n, DOWN_PIECES) + 1, lax.rem(n, DOWN_PIECES)

            @pl.when((step <= X_SIZE // 2) & (piece < UP_PIECES))
            def _():
                up_in.first_step(step, piece)

            down_in.first_step(step, piece)

        @pl.when(n >= w_first_steps)
        def _():
            m = n - w_first_steps
            group, piece = lax.div(m, DOWN_PIECES), lax.rem(m, DOWN_PIECES)

            @pl.when(piece < UP_PIECES)
            def _():
                up_in.main_step(lax.div(group, X_SIZE) + 1, lax.rem(group, X_SIZE), piece)

            down_in.main_step(lax.div(group, Z_SIZE) + 1, lax.rem(group, Z_SIZE), piece)

    waits(kvg.at[0:8], kv_pair_recv)
    for copy in locals_:
        copy.wait()

    key_at = lax.broadcasted_iota(jnp.int32, (256, 256), 0)
    later_keys = (key_at > lax.broadcasted_iota(jnp.int32, (256, 256), 1)).astype(BF16)

    def attend(query, block, diagonal):
        keys = kvg[block, 0:256, :]
        values = kvg[block, 272:528, :]
        shift = kvg[block, 256:272, :].astype(F32) * LOG2E
        shift = jnp.concatenate([shift[0:1, :], shift[1:2, :]], axis=1)
        t = lax.dot_general(qg[query], keys, NT, preferred_element_type=F32) * SCALE2 + shift
        soft = jnp.maximum(t, jnp.log2(1.0 + jnp.exp2(jnp.minimum(t, 126.0))))
        broken = soft
        if diagonal:
            q_pos = lax.rem(lax.broadcasted_iota(jnp.int32, (512, 256), 0), 256)
            visible = lax.broadcasted_iota(jnp.int32, (512, 256), 1) < q_pos
            broken = jnp.where(visible, soft, 0.0)
        later = jnp.dot(broken.astype(BF16), later_keys, preferred_element_type=F32)
        after = carry[...]
        weights = jnp.exp2((t - soft) - (later + after))
        if diagonal:
            weights = jnp.where(visible, weights, 0.0)
        acc[...] += jnp.dot(weights.astype(BF16), values, preferred_element_type=F32)
        carry[...] = after + (later[:, 0:1] + broken[:, 0:1])

    def part_copies(i):
        return (
            remote(part.at[i], part_in.at[i], part_send.at[i], part_recv.at[i], above_at(i)),
            remote(
                total_out.at[i], total_in.at[i], total_send.at[i], total_recv.at[i], above_at(i)
            ),
        )

    def above_at(i):
        return (device_at(x, lax.rem(z + 2 * (i + 1), Z_SIZE)), tp)

    def for_others(n, _):
        w_step(n)
        i, turn = lax.div(n, 16), lax.rem(n, 16)

        @pl.when(z + 2 * (i + 1) < Z_SIZE)
        def _():
            @pl.when(turn == 0)
            def _():
                waits(qg.at[i], q_recv.at[i])
                acc[...] = jnp.zeros_like(acc)
                carry[...] = jnp.zeros_like(carry)

            attend(i, 15 - turn, False)

            @pl.when(turn == 15)
            def _():
                part[i] = acc[...].astype(BF16)
                for r in range(4):
                    column = jnp.broadcast_to(carry[r * 128 : r * 128 + 128, :], (128, 128))
                    total_out[i, r] = column.T[0:8, :]
                for copy in part_copies(i):
                    copy.start()

        return 0

    def for_own(n, _):
        w_step(47 + n)

        @pl.when(here >= n)
        def _():
            attend(3, jnp.maximum(here - n, 0), False)

        return 0

    lax.fori_loop(0, 48, for_others, 0)
    acc[...] = jnp.zeros_like(acc)
    carry[...] = jnp.zeros_like(carry)
    attend(3, here, True)
    lax.fori_loop(1, 16, for_own, 0)
    for i in range(3):

        @pl.when(z >= 2 * (i + 1))
        def _():
            waits(part_in.at[i], part_recv.at[i])
            waits(total_in.at[i], total_recv.at[i])
            for r in range(4):
                rows = pl.ds(r * 128, 128)
                after = carry[rows, :]
                acc[rows, :] += jnp.exp2(-after) * part_in[i, rows, :].astype(F32)
                column = jnp.broadcast_to(total_in[i, r, 0:1, :], (128, 128)).T
                carry[rows, :] = after + column[:, 0:1]

    for d in (1, 2, 3):
        source = lax.rem(tp + 4 - d, 4)
        block = owg.at[source, core]
        remote(block, block, ow_send.at[d - 1], ow_recv.at[d - 1], partner).wait_recv()
        remote(block, block, ow_pair_send, ow_pair_recv, partner).start()
    for h in range(2):
        mixed = acc[pl.ds(h * 256, 256), :]
        power = jnp.mean(mixed * mixed, axis=1, keepdims=True)
        lanes = slice(h * 128, h * 128 + 128)
        attg[tp, :, lanes] = (mixed * lax.rsqrt(power + EPS) * gain_ref[0:1, lanes]).astype(BF16)
    for d in (2, 1, 3):
        remote(
            attg.at[tp], attg.at[tp], att_send.at[d - 1], att_recv.at[d - 1], peers[d - 1]
        ).start()
    lax.fori_loop(63, w_steps, lambda n, _: (w_step(n), 0)[1], 0)
    waits(owg.at[0:3, 0], ow_pair_recv)
    for d in (1, 2, 3):
        block = resg.at[tp]
        remote(block, block, res_send.at[d - 1], res_recv.at[d - 1], peers[d - 1]).wait_recv()
    for d in (1, 2, 3):
        block = attg.at[tp]
        remote(block, block, att_send.at[d - 1], att_recv.at[d - 1], peers[d - 1]).wait_recv()

    squares = jnp.zeros((256, 1), F32)
    for b in range(4):
        total = resg[b].astype(F32)
        for g in range(4):
            weight = owg[g, b // 2, :, (b % 2) * 512 : (b % 2) * 512 + 512]
            total = total + jnp.dot(attg[g], weight, preferred_element_type=F32)
        hidden = total.astype(BF16)
        hid[b] = hidden
        wide = hidden.astype(F32)
        squares = squares + jnp.sum(wide * wide, axis=1, keepdims=True)
    inverse = lax.rsqrt(squares / 2048.0 + EPS)
    for b in range(4):
        mi[:, b * 512 : b * 512 + 512] = (hid[b].astype(F32) * inverse * mg_ref[b]).astype(BF16)

    waits(wg.at[0:4], pair_recv.at[0])
    for b in range(4):
        lifted = jnp.dot(mi[...], wg[(5, 6, 7, 4)[b]], preferred_element_type=F32)
        lifted = jnp.maximum(lifted, 0.0)
        act[b] = (lifted * lifted).astype(BF16)

    def down(owner):
        rows = pl.ds(pl.multiple_of(owner * 512, 512), 512)
        total = jnp.zeros((256, 512), F32)
        for b in range(4):
            total = total + lax.dot_general(
                act[b], wg[b, rows, :], NT, preferred_element_type=F32
            )
        return total

    for d in (2, 1, 3):
        rs_out[d - 1] = down(lax.rem(tp + d, 4)).astype(BF16)
        remote(
            rs_out.at[d - 1], rs_in.at[d - 1], rs_send.at[d - 1], rs_recv.at[d - 1], peers[d - 1]
        ).start()
    own_part[...] = down(tp) + hid[tp].astype(F32)
    for d in (1, 3, 2):
        remote(
            rs_out.at[d - 1], rs_in.at[d - 1], rs_send.at[d - 1], rs_recv.at[d - 1], peers[d - 1]
        ).wait_recv()
    out_ref[...] = (
        own_part[...] + rs_in[0].astype(F32) + rs_in[1].astype(F32) + rs_in[2].astype(F32)
    ).astype(BF16)

    for gather in (up_in, down_in):
        for phase in range(2):
            for d in range(2):
                waits(wg.at[0, 0 : 32 * gather.sent(phase, d), :], gather.sem(phase, d))
    waits(wg.at[0:4], pair_send.at[0])
    waits(kvg.at[0], kv_send.at[2])
    for d in range(2):
        waits(kvg.at[0:3], kv_send.at[d])
    waits(kvg.at[0:8], kv_pair_send)
    for i in range(3):

        @pl.when(z >= 2 * (i + 1))
        def _():
            waits(qg.at[i], q_send.at[i])

        @pl.when(z + 2 * (i + 1) < Z_SIZE)
        def _():
            waits(part.at[i], part_send.at[i])
            waits(total_out.at[i], total_send.at[i])

    waits(owg.at[0:3, 0], ow_pair_send)
    for d in (1, 2, 3):
        waits(res_ref, res_send.at[d - 1])
        waits(owg.at[0, 0], ow_send.at[d - 1])
        waits(attg.at[0], att_send.at[d - 1])
        waits(rs_out.at[d - 1], rs_send.at[d - 1])


def body(
    residual, queries, key_rows, value_rows, break_shift, head_gain, out_weight, mlp_gain,
    up_weight, down_weight,
):
    shift = jnp.pad(break_shift.reshape(2, 128), ((0, 14), (0, 0)))
    keys_values = jnp.concatenate([key_rows, shift, value_rows], axis=0)
    vmem = pltpu.VMEM
    dma = pltpu.SemaphoreType.DMA
    return pl.pallas_call(
        kernel,
        out_shape=jax.ShapeDtypeStruct((256, 512), BF16),
        in_specs=[pl.BlockSpec(memory_space=vmem)] * 8,
        out_specs=pl.BlockSpec(memory_space=vmem),
        scratch_shapes=[
            vmem((16, KV_ROWS, 128), BF16),
            vmem((8, 2048, 512), BF16),
            vmem((4, 2, 256, 1024), BF16),
            vmem((4, 256, 512), BF16),
            vmem((4, 256, 256), BF16),
            vmem((4, 512, 128), BF16),
            vmem((3, 512, 128), BF16),
            vmem((3, 4, 8, 128), F32),
            vmem((3, 512, 128), BF16),
            vmem((3, 4, 8, 128), F32),
            vmem((512, 128), F32),
            vmem((512, 1), F32),
            vmem((4, 256, 512), BF16),
            vmem((256, 2048), BF16),
            vmem((4, 256, 512), BF16),
            vmem((3, 256, 512), BF16),
            vmem((3, 256, 512), BF16),
            vmem((256, 512), F32),
            dma((KV_PIECES,)),
            dma((2, 2, 2, KV_PIECES)),
            dma((3,)),
            dma,
            dma,
            dma((3,)),
            dma((3,)),
            dma((3,)),
            dma((3,)),
            dma((3,)),
            dma((3,)),
            dma((2, 2, UP_PIECES)),
            dma((2, 4, X_SIZE, UP_PIECES)),
            dma((2, 4, DOWN_PIECES)),
            dma((2, 2, Z_SIZE, DOWN_PIECES)),
            dma((8,)),
            dma((1,)),
            dma((1,)),
            dma((14,)),
            dma((3,)),
            dma((3,)),
            dma,
            dma,
            dma((3,)),
            dma((3,)),
            dma((3,)),
            dma((3,)),
            dma((3,)),
            dma((3,)),
        ],
        compiler_params=pltpu.CompilerParams(
            collective_id=0, has_side_effects=True, vmem_limit_bytes=60 * 1024 * 1024
        ),
        name="layer",
    )(
        residual, queries, keys_values, head_gain.reshape(1, 256), out_weight,
        mlp_gain.reshape(4, 1, 512), up_weight, down_weight.T,
    )


def solution(mesh):
    in_specs = (
        P("sp", "tp"),
        P("sp", "tp"),
        P("sp", "tp"),
        P("sp", "tp"),
        P("tp", "sp"),
        P("tp"),
        P("tp", None),
        P(),
        P("sp", "tp"),
        P("tp", "sp"),
    )
    return jax.shard_map(
        body, mesh=mesh, in_specs=in_specs, out_specs=P("sp", "tp"), check_vma=False
    )
```

```python
import functools
import math

import jax
import jax.numpy as jnp
from jax import lax
from jax.experimental import pallas as pl
from jax.experimental.pallas import tpu as pltpu
from jax.sharding import PartitionSpec as P

MESH = pl.DeviceIdType.MESH
HEAD_DIM = 128
EPS = 1e-06
LOG2E = 1.4426950408889634
SCALE2 = LOG2E / math.sqrt(HEAD_DIM)
NT = (((1,), (1,)), ((), ()))
F32 = jnp.float32
BF16 = jnp.bfloat16
KV_ROWS = 528
KV_PIECES = 3
KV_PIECE = KV_ROWS // KV_PIECES
UP_PIECES = 3
DOWN_PIECES = 5
X_SIZE, Z_SIZE = 4, 8


def offset_of(k, size):
    return jnp.where(lax.rem(k, 2) == 1, lax.div(k + 1, 2), lax.rem(size - lax.div(k, 2), size))


def last_step(size, direction, even):
    return size // 2 - jnp.where(even == (direction == 0), 0, 1)


def kernel(
    res_ref, q_ref, k_ref, v_ref, shift_ref, gain_ref, ow_ref, mg_ref, up_ref, dn_ref, out_ref,
    kv_ref, kvg, wg, owg, resg, attg, qg, part, total_out, part_in, total_in, acc, carry, hid, mi, act, rs_out, rs_in, relay_in, kept, own_part,
    row_recv, side_recv, kv_send, kv_pair_send, kv_pair_recv, q_send, q_recv,
    part_send, part_recv, total_send, total_recv,
    ua_recv, um_recv, da_recv, dm_recv, gather_send, pair_send, pair_recv,
    local_sem, ow_send, ow_recv, ow_pair_send, ow_pair_recv, res_send, res_recv,
    att_send, att_recv, rs_send, rs_recv,
):
    sp = lax.axis_index("sp")
    tp = lax.axis_index("tp")
    core = lax.rem(sp, 2)
    chip = lax.div(sp, 2)
    x, z = lax.rem(chip, 4), lax.div(chip, 4)
    partner = (sp + 1 - 2 * core, tp)

    def device_at(x, z):
        return 2 * (X_SIZE * z + x) + core

    x_sides = [(device_at(lax.rem(x + d, X_SIZE), z), tp) for d in (1, X_SIZE - 1)]
    z_sides = [(device_at(x, lax.rem(z + d, Z_SIZE)), tp) for d in (1, Z_SIZE - 1)]
    peers = [(sp, lax.rem(tp + d, 4)) for d in (1, 2, 3)]
    z_others = [(device_at(x, lax.rem(z + d, Z_SIZE)), tp) for d in range(1, Z_SIZE)]
    everyone = x_sides + z_others + [partner] + peers

    kv_ref[0:256, :] = k_ref[...]
    kv_ref[272:528, :] = v_ref[...]
    shifts = shift_ref[...].astype(F32)
    shifts = [shifts[:, 0:128], shifts[:, 128:256], jnp.zeros((14, 128), F32)]
    kv_ref[256:272, :] = jnp.concatenate(shifts, axis=0).astype(BF16)

    barrier = pltpu.get_barrier_semaphore()
    for device in everyone:
        pl.semaphore_signal(barrier, inc=1, device_id=device, device_id_type=MESH)
    pl.semaphore_wait(barrier, len(everyone))

    def remote(src, dst, send_sem, recv_sem, device):
        return pltpu.make_async_remote_copy(
            src_ref=src, dst_ref=dst, send_sem=send_sem, recv_sem=recv_sem,
            device_id=device, device_id_type=MESH,
        )

    def waits(ref, sem):
        pltpu.make_async_copy(ref, ref, sem).wait()

    def w_slot(first):
        def slot(origin, piece):
            return wg.at[first + piece, pl.ds(pl.multiple_of(origin * 32, 32), 32), :]

        return slot

    def w_source(page):
        ref, block = (dn_ref, page) if page < 4 else (up_ref, (3, 0, 1, 2)[page - 4])
        return ref.at[:, pl.ds(block * 512, 512)]

    class Gather:
        def __init__(self, number, x_first, pieces, slot, sources, first_recv, main_recv, pair):
            self.x_first, self.pieces, self.slot, self.sources = x_first, pieces, slot, sources
            self.first_recv, self.main_recv, self.pair = first_recv, main_recv, pair
            self.first_size, self.main_size = (X_SIZE, Z_SIZE) if x_first else (Z_SIZE, X_SIZE)
            self.first_to, self.main_to = (x_sides, z_sides) if x_first else (z_sides, x_sides)
            self.sem = lambda phase, d: gather_send.at[number * 4 + phase * 2 + d]

        def origin(self, first, main):
            first_at, main_at = (x, z) if self.x_first else (z, x)
            a = lax.rem(first_at + first, self.first_size)
            b = lax.rem(main_at + main, self.main_size)
            return device_at(a, b) if self.x_first else device_at(b, a)

        def send_first(self, src, dst, d, step, piece):
            return remote(
                src, dst, self.sem(0, d), self.first_recv.at[d, step - 1, piece], self.first_to[d]
            )

        def send_main(self, src, dst, d, step, k, piece):
            return remote(
                src, dst, self.sem(1, d), self.main_recv.at[d, step - 1, k, piece], self.main_to[d]
            )

        def to_partner(self, src, dst):
            remote(src, dst, pair_send.at[self.pair], pair_recv.at[self.pair], partner).start()

        def own_first(self):
            for piece in range(self.pieces):
                src, dst = self.sources[piece], self.slot(sp, piece)
                for d in range(2):
                    self.send_first(src, dst, d, 1, piece).start()

        def own_main(self):
            for piece in range(self.pieces):
                src, dst = self.sources[piece], self.slot(sp, piece)
                for d in range(2):
                    self.send_main(src, dst, d, 1, 0, piece).start()

        def own_near(self):
            for piece in range(self.pieces):
                src, dst = self.sources[piece], self.slot(sp, piece)
                self.to_partner(src, dst)
                keep(src, dst)

        def first_step(self, step, piece):
            for d in range(2):
                last = last_step(self.first_size, d, lax.rem(piece, 2) == 0)
                ahead = self.first_size - step if d == 0 else step
                k = jnp.minimum(2 * step, self.first_size - 1) if d == 0 else 2 * step - 1
                block = self.slot(self.origin(ahead, 0), piece)

                @pl.when(step <= last)
                def _():
                    self.send_first(block, block, d, step, piece).wait_recv()

                @pl.when(step < last)
                def _():
                    self.send_first(block, block, d, step + 1, piece).start()

                @pl.when(step <= last)
                def _():
                    for e in range(2):
                        self.send_main(block, block, e, 1, k, piece).start()
                    self.to_partner(block, block)

        def main_step(self, step, k, piece):
            for d in range(2):
                last = last_step(self.main_size, d, lax.rem(k, 2) == 0)
                ahead = self.main_size - step if d == 0 else step
                block = self.slot(self.origin(offset_of(k, self.first_size), ahead), piece)

                @pl.when(step <= last)
                def _():
                    self.send_main(block, block, d, step, k, piece).wait_recv()

                @pl.when(step < last)
                def _():
                    self.send_main(block, block, d, step + 1, k, piece).start()

                @pl.when(step <= last)
                def _():
                    self.to_partner(block, block)

        def sent(self, phase, d):
            if phase == 0:
                long = [(piece % 2 == 0) == (d == 0) for piece in range(self.pieces)]
                return sum(self.first_size // 2 - (not far) for far in long)
            return self.pieces * self.first_size * (self.main_size - 1) // 2

    locals_ = []

    def keep(src, dst):
        copy = pltpu.make_async_copy(src, dst, local_sem.at[len(locals_)])
        copy.start()
        locals_.append(copy)

    up_in = Gather(
        0, True, UP_PIECES, w_slot(5), [w_source(p) for p in (5, 6, 7)], ua_recv, um_recv, 0
    )
    down_in = Gather(
        1, False, DOWN_PIECES, w_slot(0), [w_source(p) for p in range(5)], da_recv, dm_recv, 0
    )

    row = lax.rem(z, 2)
    here = (row * X_SIZE + x) * 2 + core
    beside = (device_at(x, z + 1 - 2 * row), tp)

    def kv_slot(at_row, at_x, piece, at_core=core):
        start = pl.multiple_of(piece * KV_PIECE, KV_PIECE)
        return kvg.at[(at_row * X_SIZE + at_x) * 2 + at_core, pl.ds(start, KV_PIECE), :]

    def kv_source(piece):
        return kv_ref.at[pl.ds(pl.multiple_of(piece * KV_PIECE, KV_PIECE), KV_PIECE), :]

    def to_row(src, piece):
        return remote(src, kv_slot(row, x, piece), kv_send.at[2], row_recv.at[piece], beside)

    def to_side(src, d, step, at_row, at_x, piece):
        recv = side_recv.at[d, step - 1, at_row, piece]
        return remote(src, kv_slot(at_row, at_x, piece), kv_send.at[d], recv, x_sides[d])

    def to_core(src, at_row, at_x, piece):
        remote(src, kv_slot(at_row, at_x, piece), kv_pair_send, kv_pair_recv, partner).start()

    def send_own(piece, _):
        src = kv_source(piece)
        to_row(src, piece).start()
        for d in range(2):
            to_side(src, d, 1, row, x, piece).start()
        to_core(src, row, x, piece)
        return 0

    lax.fori_loop(0, KV_PIECES, send_own, 0)
    keep(kv_ref, kvg.at[here])
    pair_row = lax.div(z, 2)

    def server_of(p):
        odd = z <= p + 4
        return jnp.where(odd, 2 * p + 1, 2 * p), jnp.where(odd, z - 2 * p - 2, 7 - z)

    def client_at(i):
        return (device_at(x, jnp.where(lax.rem(z, 2) == 1, z + 1 + i, 7 - i)), tp)

    for p in range(3):

        @pl.when(pair_row > p)
        def _():
            at, i = server_of(p)
            for h in range(2):
                remote(
                    q_ref.at[:, pl.ds(h * 128, 128)], qg.at[i, pl.ds(h * 256, 256), :],
                    q_send.at[p], q_recv.at[i], (device_at(x, at), tp),
                ).start()

    for h in range(2):
        keep(q_ref.at[:, pl.ds(h * 128, 128)], qg.at[3, pl.ds(h * 256, 256), :])

    def from_row(piece, _):
        at_row = 1 - row
        block = kv_slot(at_row, x, piece)
        remote(block, block, kv_send.at[2], row_recv.at[piece], beside).wait_recv()
        for d in range(2):
            to_side(block, d, 1, at_row, x, piece).start()
        to_core(block, at_row, x, piece)
        return 0

    def from_side(at_row, step, piece):
        for d in range(2):
            at_x = lax.rem(x + (X_SIZE - step if d == 0 else step), X_SIZE)
            block = kv_slot(at_row, at_x, piece)
            long = at_row == d

            def arrives():
                recv = side_recv.at[d, step - 1, at_row, piece]
                remote(block, block, kv_send.at[d], recv, x_sides[d]).wait_recv()

            if step == 1:
                arrives()

                @pl.when(long)
                def _():
                    to_side(block, d, 2, at_row, at_x, piece).start()

                to_core(block, at_row, at_x, piece)
            else:

                @pl.when(long)
                def _():
                    arrives()
                    to_core(block, at_row, at_x, piece)

    w_first_steps = DOWN_PIECES * Z_SIZE // 2
    w_steps = w_first_steps + DOWN_PIECES * 16

    def w_step(n):
        @pl.when(n < w_first_steps)
        def _():
            step, piece = lax.div(n, DOWN_PIECES) + 1, lax.rem(n, DOWN_PIECES)

            @pl.when((step <= X_SIZE // 2) & (piece < UP_PIECES))
            def _():
                up_in.first_step(step, piece)

            down_in.first_step(step, piece)

        @pl.when(n >= w_first_steps)
        def _():
            m = n - w_first_steps
            group, piece = lax.div(m, DOWN_PIECES), lax.rem(m, DOWN_PIECES)

            @pl.when(piece < UP_PIECES)
            def _():
                up_in.main_step(lax.div(group, X_SIZE) + 1, lax.rem(group, X_SIZE), piece)

            down_in.main_step(lax.div(group, Z_SIZE) + 1, lax.rem(group, Z_SIZE), piece)

    def w_loop(first, last):
        lax.fori_loop(first, last, lambda n, _: (w_step(n), 0)[1], 0)

    def near_side(piece, _):
        from_side(row, 1, piece)
        return 0

    def far_sides(piece, _):
        from_side(1 - row, 1, piece)
        from_side(row, 2, piece)
        return 0

    def last_side(piece, _):
        from_side(1 - row, 2, piece)
        return 0

    lax.fori_loop(0, KV_PIECES, from_row, 0)
    lax.fori_loop(0, KV_PIECES, near_side, 0)
    up_in.own_first()
    up_in.own_main()
    down_in.own_first()
    down_in.own_main()
    up_in.own_near()
    down_in.own_near()
    lax.fori_loop(0, KV_PIECES, far_sides, 0)
    lax.fori_loop(0, KV_PIECES, last_side, 0)
    half = pl.ds(pl.multiple_of(core * 1024, 1024), 1024)
    for d in (1, 2, 3):
        remote(res_ref, resg.at[tp], res_send.at[d - 1], res_recv.at[d - 1], peers[d - 1]).start()
    for d in (1, 2, 3):
        remote(
            ow_ref.at[:, half], owg.at[tp, core], ow_send.at[d - 1], ow_recv.at[d - 1], peers[d - 1]
        ).start()
    for c in range(2):
        keep(ow_ref.at[:, pl.ds(c * 1024, 1024)], owg.at[tp, c])
    keep(res_ref, resg.at[tp])
    waits(kvg.at[0:8], kv_pair_recv)
    for copy in locals_:
        copy.wait()

    key_at = lax.broadcasted_iota(jnp.int32, (256, 256), 0)
    later_keys = (key_at > lax.broadcasted_iota(jnp.int32, (256, 256), 1)).astype(BF16)

    def attend(query, block, diagonal):
        keys = kvg[block, 0:256, :]
        values = kvg[block, 272:528, :]
        shift = kvg[block, 256:272, :].astype(F32) * LOG2E
        shift = jnp.concatenate([shift[0:1, :], shift[1:2, :]], axis=1)
        t = lax.dot_general(qg[query], keys, NT, preferred_element_type=F32) * SCALE2 + shift
        soft = jnp.maximum(t, jnp.log2(1.0 + jnp.exp2(jnp.minimum(t, 126.0))))
        broken = soft
        if diagonal:
            q_pos = lax.rem(lax.broadcasted_iota(jnp.int32, (512, 256), 0), 256)
            visible = lax.broadcasted_iota(jnp.int32, (512, 256), 1) < q_pos
            broken = jnp.where(visible, soft, 0.0)
        later = jnp.dot(broken.astype(BF16), later_keys, preferred_element_type=F32)
        after = carry[...]
        weights = jnp.exp2((t - soft) - (later + after))
        if diagonal:
            weights = jnp.where(visible, weights, 0.0)
        acc[...] += jnp.dot(weights.astype(BF16), values, preferred_element_type=F32)
        carry[...] = after + (later[:, 0:1] + broken[:, 0:1])

    def part_copies(i):
        return (
            remote(
                part.at[i], part_in.at[pair_row], part_send.at[i], part_recv.at[pair_row], client_at(i)
            ),
            remote(
                total_out.at[i], total_in.at[pair_row], total_send.at[i],
                total_recv.at[pair_row], client_at(i),
            ),
        )

    busy = 2 * w_first_steps

    def for_others(n, _):
        early = n < busy
        w_loop(
            jnp.where(early, lax.div(n + 1, 2), 2 * n + w_first_steps - 2 * busy),
            jnp.where(early, lax.div(n + 2, 2), 2 * n + w_first_steps - 2 * busy + 2),
        )
        i, turn = lax.div(n, 16), lax.rem(n, 16)

        @pl.when(pair_row + i < 3)
        def _():
            @pl.when(turn == 0)
            def _():
                waits(qg.at[i], q_recv.at[i])
                acc[...] = jnp.zeros_like(acc)
                carry[...] = jnp.zeros_like(carry)

            attend(i, 15 - turn, False)

            @pl.when(turn == 15)
            def _():
                part[i] = acc[...].astype(BF16)
                for r in range(4):
                    column = jnp.broadcast_to(carry[r * 128 : r * 128 + 128, :], (128, 128))
                    total_out[i, r] = column.T[0:8, :]
                for copy in part_copies(i):
                    copy.start()

        return 0

    def for_own(n, _):
        w_loop(w_others + 2 * n - 2, w_others + 2 * n)

        @pl.when(here >= n)
        def _():
            attend(3, jnp.maximum(here - n, 0), False)

        return 0

    w_others = w_first_steps + 2 * (48 - busy)
    lax.fori_loop(0, 48, for_others, 0)
    acc[...] = jnp.zeros_like(acc)
    carry[...] = jnp.zeros_like(carry)
    attend(3, here, True)
    lax.fori_loop(1, 16, for_own, 0)
    for p in (2, 1, 0):

        @pl.when(pair_row > p)
        def _():
            waits(part_in.at[p], part_recv.at[p])
            waits(total_in.at[p], total_recv.at[p])
            for r in range(4):
                rows = pl.ds(r * 128, 128)
                after = carry[rows, :]
                acc[rows, :] += jnp.exp2(-after) * part_in[p, rows, :].astype(F32)
                column = jnp.broadcast_to(total_in[p, r, 0:1, :], (128, 128)).T
                carry[rows, :] = after + column[:, 0:1]

    for d in (1, 2, 3):
        source = lax.rem(tp + 4 - d, 4)
        block = owg.at[source, core]
        remote(block, block, ow_send.at[d - 1], ow_recv.at[d - 1], partner).wait_recv()
        remote(block, block, ow_pair_send, ow_pair_recv, partner).start()
    for h in range(2):
        mixed = acc[pl.ds(h * 256, 256), :]
        power = jnp.mean(mixed * mixed, axis=1, keepdims=True)
        lanes = slice(h * 128, h * 128 + 128)
        attg[tp, :, lanes] = (mixed * lax.rsqrt(power + EPS) * gain_ref[0:1, lanes]).astype(BF16)
    for d in (2, 1, 3):
        remote(
            attg.at[tp], attg.at[tp], att_send.at[d - 1], att_recv.at[d - 1], peers[d - 1]
        ).start()
    w_loop(w_others + 30, w_steps - 14)
    waits(owg.at[0:3, 0], ow_pair_recv)
    for d in (1, 2, 3):
        block = resg.at[tp]
        remote(block, block, res_send.at[d - 1], res_recv.at[d - 1], peers[d - 1]).wait_recv()
    for d in (1, 2, 3):
        block = attg.at[tp]
        remote(block, block, att_send.at[d - 1], att_recv.at[d - 1], peers[d - 1]).wait_recv()

    squares = jnp.zeros((256, 1), F32)
    for b in range(4):
        total = resg[b].astype(F32)
        for g in range(4):
            weight = owg[g, b // 2, :, (b % 2) * 512 : (b % 2) * 512 + 512]
            total = total + jnp.dot(attg[g], weight, preferred_element_type=F32)
        hidden = total.astype(BF16)
        hid[b] = hidden
        wide = hidden.astype(F32)
        squares = squares + jnp.sum(wide * wide, axis=1, keepdims=True)
    inverse = lax.rsqrt(squares / 2048.0 + EPS)
    for b in range(4):
        mi[:, b * 512 : b * 512 + 512] = (hid[b].astype(F32) * inverse * mg_ref[b]).astype(BF16)

    w_loop(w_steps - 14, w_steps)
    waits(wg.at[0:4], pair_recv.at[0])
    for b in range(4):
        lifted = jnp.dot(mi[...], wg[(5, 6, 7, 4)[b]], preferred_element_type=F32)
        lifted = jnp.maximum(lifted, 0.0)
        act[b] = (lifted * lifted).astype(BF16)

    def down(owner):
        rows = pl.ds(pl.multiple_of(owner * 512, 512), 512)
        total = jnp.zeros((256, 512), F32)
        for b in range(4):
            total = total + lax.dot_general(
                act[b], wg[b, rows, :], NT, preferred_element_type=F32
            )
        return total

    first, second = pl.ds(0, 128), pl.ds(128, 128)

    def to_peer(n, src, dst, d):
        return remote(src, dst, rs_send.at[n], rs_recv.at[n], peers[d - 1])

    def hand_over():
        return (
            to_peer(0, rs_out.at[0, first], relay_in.at[0], 1),
            to_peer(1, rs_out.at[0, second], relay_in.at[1], 3),
        )

    def direct():
        return (
            to_peer(2, rs_out.at[1, second], rs_in.at[0, second], 1),
            to_peer(3, rs_out.at[2, first], rs_in.at[1, first], 3),
        )

    def combined():
        return (
            to_peer(4, rs_out.at[1, first], rs_in.at[0, first], 1),
            to_peer(5, rs_out.at[2, second], rs_in.at[1, second], 3),
        )

    rs_out[0] = down(lax.rem(tp + 2, 4)).astype(BF16)
    for copy in hand_over():
        copy.start()
    share = down(lax.rem(tp + 1, 4))
    kept[0] = share[0:128]
    rs_out[1, second, :] = share[128:256].astype(BF16)
    direct()[0].start()
    share = down(lax.rem(tp + 3, 4))
    kept[1] = share[128:256]
    rs_out[2, first, :] = share[0:128].astype(BF16)
    direct()[1].start()
    own_part[...] = down(tp) + hid[tp].astype(F32)
    for n in range(2):
        hand_over()[n].wait_recv()
        rs_out[1 + n, (first, second)[n], :] = (kept[n] + relay_in[n].astype(F32)).astype(BF16)
        combined()[n].start()
    for copy in direct() + combined():
        copy.wait_recv()
    out_ref[...] = (own_part[...] + rs_in[0].astype(F32) + rs_in[1].astype(F32)).astype(BF16)

    for n in range(6):
        waits(rs_out.at[0, first], rs_send.at[n])
    for gather in (up_in, down_in):
        for phase in range(2):
            for d in range(2):
                waits(wg.at[0, 0 : 32 * gather.sent(phase, d), :], gather.sem(phase, d))
    waits(wg.at[0:4], pair_send.at[0])
    waits(kvg.at[0], kv_send.at[2])
    for d in range(2):
        waits(kvg.at[0:3], kv_send.at[d])
    waits(kvg.at[0:8], kv_pair_send)
    for i in range(3):

        @pl.when(pair_row > i)
        def _():
            waits(qg.at[i], q_send.at[i])

        @pl.when(pair_row + i < 3)
        def _():
            waits(part.at[i], part_send.at[i])
            waits(total_out.at[i], total_send.at[i])

    waits(owg.at[0:3, 0], ow_pair_send)
    for d in (1, 2, 3):
        waits(res_ref, res_send.at[d - 1])
        waits(owg.at[0, 0], ow_send.at[d - 1])
        waits(attg.at[0], att_send.at[d - 1])


def body(
    residual, queries, key_rows, value_rows, break_shift, head_gain, out_weight, mlp_gain,
    up_weight, down_weight,
):
    vmem = pltpu.VMEM
    dma = pltpu.SemaphoreType.DMA
    return pl.pallas_call(
        kernel,
        out_shape=jax.ShapeDtypeStruct((256, 512), BF16),
        in_specs=[pl.BlockSpec(memory_space=vmem)] * 10,
        out_specs=pl.BlockSpec(memory_space=vmem),
        scratch_shapes=[
            vmem((KV_ROWS, 128), BF16),
            vmem((16, KV_ROWS, 128), BF16),
            vmem((8, 2048, 512), BF16),
            vmem((4, 2, 256, 1024), BF16),
            vmem((4, 256, 512), BF16),
            vmem((4, 256, 256), BF16),
            vmem((4, 512, 128), BF16),
            vmem((3, 512, 128), BF16),
            vmem((3, 4, 8, 128), F32),
            vmem((3, 512, 128), BF16),
            vmem((3, 4, 8, 128), F32),
            vmem((512, 128), F32),
            vmem((512, 1), F32),
            vmem((4, 256, 512), BF16),
            vmem((256, 2048), BF16),
            vmem((4, 256, 512), BF16),
            vmem((3, 256, 512), BF16),
            vmem((2, 256, 512), BF16),
            vmem((2, 128, 512), BF16),
            vmem((2, 128, 512), F32),
            vmem((256, 512), F32),
            dma((KV_PIECES,)),
            dma((2, 2, 2, KV_PIECES)),
            dma((3,)),
            dma,
            dma,
            dma((3,)),
            dma((3,)),
            dma((3,)),
            dma((3,)),
            dma((3,)),
            dma((3,)),
            dma((2, 2, UP_PIECES)),
            dma((2, 4, X_SIZE, UP_PIECES)),
            dma((2, 4, DOWN_PIECES)),
            dma((2, 2, Z_SIZE, DOWN_PIECES)),
            dma((8,)),
            dma((1,)),
            dma((1,)),
            dma((14,)),
            dma((3,)),
            dma((3,)),
            dma,
            dma,
            dma((3,)),
            dma((3,)),
            dma((3,)),
            dma((3,)),
            dma((6,)),
            dma((6,)),
        ],
        compiler_params=pltpu.CompilerParams(
            collective_id=0, has_side_effects=True, vmem_limit_bytes=60 * 1024 * 1024
        ),
        name="layer",
    )(
        residual, queries, key_rows, value_rows, break_shift, head_gain.reshape(1, 256), out_weight,
        mlp_gain.reshape(4, 1, 512), up_weight, down_weight.T,
    )


def solution(mesh):
    in_specs = (
        P("sp", "tp"),
        P("sp", "tp"),
        P("sp", "tp"),
        P("sp", "tp"),
        P("tp", "sp"),
        P("tp"),
        P("tp", None),
        P(),
        P("sp", "tp"),
        P("tp", "sp"),
    )
    return jax.shard_map(
        body, mesh=mesh, in_specs=in_specs, out_specs=P("sp", "tp"), check_vma=False
    )
```

```python
import functools
import math

import jax
import jax.numpy as jnp
from jax import lax
from jax.experimental import pallas as pl
from jax.experimental.pallas import tpu as pltpu
from jax.sharding import PartitionSpec as P

MESH = pl.DeviceIdType.MESH
HEAD_DIM = 128
EPS = 1e-06
LOG2E = 1.4426950408889634
SCALE2 = LOG2E / math.sqrt(HEAD_DIM)
NT = (((1,), (1,)), ((), ()))
F32 = jnp.float32
BF16 = jnp.bfloat16
KV_ROWS = 528
KV_PIECES = 3
KV_PIECE = KV_ROWS // KV_PIECES
UP_PIECES = 3
DOWN_PIECES = 5
X_SIZE, Z_SIZE = 4, 8


def offset_of(k, size):
    return jnp.where(lax.rem(k, 2) == 1, lax.div(k + 1, 2), lax.rem(size - lax.div(k, 2), size))


def last_step(size, direction, even):
    return size // 2 - jnp.where(even == (direction == 0), 0, 1)


def kernel(
    res_ref, q_ref, k_ref, v_ref, shift_ref, gain_ref, ow_ref, mg_ref, up_ref, dn_ref, out_ref,
    kv_ref, kvg, wg, owg, resg, attg, qg, part, total_out, part_in, total_in, acc, carry, hid, mi, act, rs_out, rs_in, relay_in, kept, own_part,
    row_recv, side_recv, kv_send, kv_pair_send, kv_pair_recv, q_send, q_recv,
    part_send, part_recv, total_send, total_recv,
    ua_recv, um_recv, da_recv, dm_recv, gather_send, pair_send, pair_recv,
    local_sem, ow_send, ow_recv, ow_pair_send, ow_pair_recv, res_send, res_recv,
    att_send, att_recv, rs_send, rs_recv,
):
    sp = lax.axis_index("sp")
    tp = lax.axis_index("tp")
    core = lax.rem(sp, 2)
    chip = lax.div(sp, 2)
    x, z = lax.rem(chip, 4), lax.div(chip, 4)
    partner = (sp + 1 - 2 * core, tp)

    def device_at(x, z):
        return 2 * (X_SIZE * z + x) + core

    x_sides = [(device_at(lax.rem(x + d, X_SIZE), z), tp) for d in (1, X_SIZE - 1)]
    z_sides = [(device_at(x, lax.rem(z + d, Z_SIZE)), tp) for d in (1, Z_SIZE - 1)]
    peers = [(sp, lax.rem(tp + d, 4)) for d in (1, 2, 3)]
    z_others = [(device_at(x, lax.rem(z + d, Z_SIZE)), tp) for d in range(1, Z_SIZE)]
    everyone = x_sides + z_others + [partner] + peers

    kv_ref[0:256, :] = k_ref[...]
    kv_ref[272:528, :] = v_ref[...]
    shifts = shift_ref[...].astype(F32)
    shifts = [shifts[:, 0:128], shifts[:, 128:256], jnp.zeros((14, 128), F32)]
    kv_ref[256:272, :] = jnp.concatenate(shifts, axis=0).astype(BF16)

    barrier = pltpu.get_barrier_semaphore()
    for device in everyone:
        pl.semaphore_signal(barrier, inc=1, device_id=device, device_id_type=MESH)
    pl.semaphore_wait(barrier, len(everyone))

    def remote(src, dst, send_sem, recv_sem, device):
        return pltpu.make_async_remote_copy(
            src_ref=src, dst_ref=dst, send_sem=send_sem, recv_sem=recv_sem,
            device_id=device, device_id_type=MESH,
        )

    def waits(ref, sem):
        pltpu.make_async_copy(ref, ref, sem).wait()

    def w_slot(first):
        def slot(origin, piece):
            return wg.at[first + piece, pl.ds(pl.multiple_of(origin * 32, 32), 32), :]

        return slot

    def w_source(page):
        ref, block = (dn_ref, page) if page < 4 else (up_ref, (3, 0, 1, 2)[page - 4])
        return ref.at[:, pl.ds(block * 512, 512)]

    class Gather:
        def __init__(self, number, x_first, pieces, slot, sources, first_recv, main_recv, pair):
            self.x_first, self.pieces, self.slot, self.sources = x_first, pieces, slot, sources
            self.first_recv, self.main_recv, self.pair = first_recv, main_recv, pair
            self.first_size, self.main_size = (X_SIZE, Z_SIZE) if x_first else (Z_SIZE, X_SIZE)
            self.first_to, self.main_to = (x_sides, z_sides) if x_first else (z_sides, x_sides)
            self.sem = lambda phase, d: gather_send.at[number * 4 + phase * 2 + d]

        def origin(self, first, main):
            first_at, main_at = (x, z) if self.x_first else (z, x)
            a = lax.rem(first_at + first, self.first_size)
            b = lax.rem(main_at + main, self.main_size)
            return device_at(a, b) if self.x_first else device_at(b, a)

        def send_first(self, src, dst, d, step, piece):
            return remote(
                src, dst, self.sem(0, d), self.first_recv.at[d, step - 1, piece], self.first_to[d]
            )

        def send_main(self, src, dst, d, step, k, piece):
            return remote(
                src, dst, self.sem(1, d), self.main_recv.at[d, step - 1, k, piece], self.main_to[d]
            )

        def to_partner(self, src, dst):
            remote(src, dst, pair_send.at[self.pair], pair_recv.at[self.pair], partner).start()

        def own_first(self):
            for piece in range(self.pieces):
                src, dst = self.sources[piece], self.slot(sp, piece)
                for d in range(2):
                    self.send_first(src, dst, d, 1, piece).start()

        def own_main(self):
            for piece in range(self.pieces):
                src, dst = self.sources[piece], self.slot(sp, piece)
                for d in range(2):
                    self.send_main(src, dst, d, 1, 0, piece).start()

        def own_near(self):
            for piece in range(self.pieces):
                src, dst = self.sources[piece], self.slot(sp, piece)
                self.to_partner(src, dst)
                keep(src, dst)

        def first_step(self, step, piece):
            for d in range(2):
                last = last_step(self.first_size, d, lax.rem(piece, 2) == 0)
                ahead = self.first_size - step if d == 0 else step
                k = jnp.minimum(2 * step, self.first_size - 1) if d == 0 else 2 * step - 1
                block = self.slot(self.origin(ahead, 0), piece)

                @pl.when(step <= last)
                def _():
                    self.send_first(block, block, d, step, piece).wait_recv()

                @pl.when(step < last)
                def _():
                    self.send_first(block, block, d, step + 1, piece).start()

                @pl.when(step <= last)
                def _():
                    for e in range(2):
                        self.send_main(block, block, e, 1, k, piece).start()
                    self.to_partner(block, block)

        def main_step(self, step, k, piece):
            for d in range(2):
                last = last_step(self.main_size, d, lax.rem(k, 2) == 0)
                ahead = self.main_size - step if d == 0 else step
                block = self.slot(self.origin(offset_of(k, self.first_size), ahead), piece)

                @pl.when(step <= last)
                def _():
                    self.send_main(block, block, d, step, k, piece).wait_recv()

                @pl.when(step < last)
                def _():
                    self.send_main(block, block, d, step + 1, k, piece).start()

                @pl.when(step <= last)
                def _():
                    self.to_partner(block, block)

        def sent(self, phase, d):
            if phase == 0:
                long = [(piece % 2 == 0) == (d == 0) for piece in range(self.pieces)]
                return sum(self.first_size // 2 - (not far) for far in long)
            return self.pieces * self.first_size * (self.main_size - 1) // 2

    locals_ = []

    def keep(src, dst):
        copy = pltpu.make_async_copy(src, dst, local_sem.at[len(locals_)])
        copy.start()
        locals_.append(copy)

    up_in = Gather(
        0, True, UP_PIECES, w_slot(5), [w_source(p) for p in (5, 6, 7)], ua_recv, um_recv, 0
    )
    down_in = Gather(
        1, False, DOWN_PIECES, w_slot(0), [w_source(p) for p in range(5)], da_recv, dm_recv, 0
    )

    row = lax.rem(z, 2)
    here = (row * X_SIZE + x) * 2 + core
    beside = (device_at(x, z + 1 - 2 * row), tp)

    def kv_slot(at_row, at_x, piece, at_core=core):
        start = pl.multiple_of(piece * KV_PIECE, KV_PIECE)
        return kvg.at[(at_row * X_SIZE + at_x) * 2 + at_core, pl.ds(start, KV_PIECE), :]

    def kv_source(piece):
        return kv_ref.at[pl.ds(pl.multiple_of(piece * KV_PIECE, KV_PIECE), KV_PIECE), :]

    def to_row(src, piece):
        return remote(src, kv_slot(row, x, piece), kv_send.at[2], row_recv.at[piece], beside)

    def to_side(src, d, step, at_row, at_x, piece):
        recv = side_recv.at[d, step - 1, at_row, piece]
        return remote(src, kv_slot(at_row, at_x, piece), kv_send.at[d], recv, x_sides[d])

    def to_core(src, at_row, at_x, piece):
        remote(src, kv_slot(at_row, at_x, piece), kv_pair_send, kv_pair_recv, partner).start()

    def send_own(piece, _):
        src = kv_source(piece)
        to_row(src, piece).start()
        for d in range(2):
            to_side(src, d, 1, row, x, piece).start()
        to_core(src, row, x, piece)
        return 0

    lax.fori_loop(0, KV_PIECES, send_own, 0)
    keep(kv_ref, kvg.at[here])
    pair_row = lax.div(z, 2)

    def server_of(p):
        odd = z <= p + 4
        return jnp.where(odd, 2 * p + 1, 2 * p), jnp.where(odd, z - 2 * p - 2, 7 - z)

    def client_at(i):
        return (device_at(x, jnp.where(lax.rem(z, 2) == 1, z + 1 + i, 7 - i)), tp)

    def send_queries(turn):
        for p in range(3):
            at, i = server_of(p)

            @pl.when((pair_row > p) & (i == turn))
            def _():
                for h in range(2):
                    remote(
                        q_ref.at[:, pl.ds(h * 128, 128)], qg.at[turn, pl.ds(h * 256, 256), :],
                        q_send.at[p], q_recv.at[turn], (device_at(x, at), tp),
                    ).start()

    send_queries(0)
    for h in range(2):
        keep(q_ref.at[:, pl.ds(h * 128, 128)], qg.at[3, pl.ds(h * 256, 256), :])

    def from_row(piece, _):
        at_row = 1 - row
        block = kv_slot(at_row, x, piece)
        remote(block, block, kv_send.at[2], row_recv.at[piece], beside).wait_recv()
        for d in range(2):
            to_side(block, d, 1, at_row, x, piece).start()
        to_core(block, at_row, x, piece)
        return 0

    def from_side(at_row, step, piece):
        for d in range(2):
            at_x = lax.rem(x + (X_SIZE - step if d == 0 else step), X_SIZE)
            block = kv_slot(at_row, at_x, piece)
            long = at_row == d

            def arrives():
                recv = side_recv.at[d, step - 1, at_row, piece]
                remote(block, block, kv_send.at[d], recv, x_sides[d]).wait_recv()

            if step == 1:
                arrives()

                @pl.when(long)
                def _():
                    to_side(block, d, 2, at_row, at_x, piece).start()

                to_core(block, at_row, at_x, piece)
            else:

                @pl.when(long)
                def _():
                    arrives()
                    to_core(block, at_row, at_x, piece)

    w_first_steps = DOWN_PIECES * Z_SIZE // 2
    w_steps = w_first_steps + DOWN_PIECES * 16

    up_start = DOWN_PIECES * (X_SIZE // 2 + 1)
    up_every = up_start + UP_PIECES * X_SIZE
    up_end = up_every + 2 * UP_PIECES * (16 - X_SIZE)

    def w_step(n):
        step, piece = lax.div(n, DOWN_PIECES) + 1, lax.rem(n, DOWN_PIECES)

        @pl.when(n < w_first_steps)
        def _():
            down_in.first_step(step, piece)

        @pl.when((step > 1) & (step <= X_SIZE // 2 + 1) & (piece < UP_PIECES))
        def _():
            up_in.first_step(step - 1, piece)

        @pl.when(n >= w_first_steps)
        def _():
            group = lax.div(n - w_first_steps, DOWN_PIECES)
            down_in.main_step(lax.div(group, Z_SIZE) + 1, lax.rem(group, Z_SIZE), piece)

        @pl.when((n >= up_start) & ((n < up_every) | ((lax.rem(n, 2) == 0) & (n < up_end))))
        def _():
            m = jnp.where(n < up_every, n - up_start, UP_PIECES * X_SIZE + lax.div(n - up_every, 2))
            group = lax.div(m, UP_PIECES)
            up_in.main_step(
                lax.div(group, X_SIZE) + 1, lax.rem(group, X_SIZE), lax.rem(m, UP_PIECES)
            )

    def w_loop(first, last):
        lax.fori_loop(first, last, lambda n, _: (w_step(n), 0)[1], 0)

    def near_side(piece, _):
        from_side(row, 1, piece)
        return 0

    def far_sides(piece, _):
        from_side(1 - row, 1, piece)
        from_side(row, 2, piece)
        return 0

    def last_side(piece, _):
        from_side(1 - row, 2, piece)
        return 0

    lax.fori_loop(0, KV_PIECES, from_row, 0)
    lax.fori_loop(0, KV_PIECES, near_side, 0)
    down_in.own_first()
    up_in.own_main()
    up_in.own_near()
    down_in.own_near()
    lax.fori_loop(0, KV_PIECES, far_sides, 0)
    up_in.own_first()
    down_in.own_main()
    w_loop(0, DOWN_PIECES)
    lax.fori_loop(0, KV_PIECES, last_side, 0)
    half = pl.ds(pl.multiple_of(core * 1024, 1024), 1024)
    for d in (1, 2, 3):
        remote(res_ref, resg.at[tp], res_send.at[d - 1], res_recv.at[d - 1], peers[d - 1]).start()
    for d in (1, 2, 3):
        remote(
            ow_ref.at[:, half], owg.at[tp, core], ow_send.at[d - 1], ow_recv.at[d - 1], peers[d - 1]
        ).start()
    for c in range(2):
        keep(ow_ref.at[:, pl.ds(c * 1024, 1024)], owg.at[tp, c])
    keep(res_ref, resg.at[tp])
    waits(kvg.at[0:8], kv_pair_recv)
    for copy in locals_:
        copy.wait()

    key_at = lax.broadcasted_iota(jnp.int32, (256, 256), 0)
    later_keys = (key_at > lax.broadcasted_iota(jnp.int32, (256, 256), 1)).astype(BF16)

    def broken_of(query, block, visible=None):
        keys = kvg[block, 0:256, :]
        shift = kvg[block, 256:272, :].astype(F32) * LOG2E
        shift = jnp.concatenate([shift[0:1, :], shift[1:2, :]], axis=1)
        t = lax.dot_general(qg[query], keys, NT, preferred_element_type=F32) * SCALE2 + shift
        soft = jnp.maximum(t, jnp.log2(1.0 + jnp.exp2(jnp.minimum(t, 126.0))))
        broken = soft if visible is None else jnp.where(visible, soft, 0.0)
        later = jnp.dot(broken.astype(BF16), later_keys, preferred_element_type=F32)
        return t - soft, later, later[:, 0:1] + broken[:, 0:1]

    def attend(query, block, diagonal):
        visible = None
        if diagonal:
            q_pos = lax.rem(lax.broadcasted_iota(jnp.int32, (512, 256), 0), 256)
            visible = lax.broadcasted_iota(jnp.int32, (512, 256), 1) < q_pos
        picked, later, whole = broken_of(query, block, visible)
        after = carry[...]
        weights = jnp.exp2(picked - (later + after))
        if diagonal:
            weights = jnp.where(visible, weights, 0.0)
        values = kvg[block, 272:528, :]
        acc[...] += jnp.dot(weights.astype(BF16), values, preferred_element_type=F32)
        carry[...] = after + whole

    def attend_two(query, newer):
        picked, later, whole = broken_of(query, newer)
        older_picked, older_later, older_whole = broken_of(query, newer - 1)
        after = carry[...]
        older_after = after + whole
        weights = [
            jnp.exp2(older_picked - (older_later + older_after)).astype(BF16),
            jnp.exp2(picked - (later + after)).astype(BF16),
        ]
        values = [kvg[newer - 1, 272:528, :], kvg[newer, 272:528, :]]
        acc[...] += jnp.dot(
            jnp.concatenate(weights, axis=1),
            jnp.concatenate(values, axis=0),
            preferred_element_type=F32,
        )
        carry[...] = older_after + older_whole

    def part_copies(i):
        return (
            remote(
                part.at[i], part_in.at[pair_row], part_send.at[i], part_recv.at[pair_row], client_at(i)
            ),
            remote(
                total_out.at[i], total_in.at[pair_row], total_send.at[i],
                total_recv.at[pair_row], client_at(i),
            ),
        )

    busy = w_first_steps - DOWN_PIECES

    def for_others(n, _):
        w_loop(
            DOWN_PIECES + lax.div(n * busy + 23, 24), DOWN_PIECES + lax.div((n + 1) * busy + 23, 24)
        )
        for later in (1, 2):

            @pl.when(n == 6 * later - 4)
            def _():
                send_queries(later)

        i, turn = lax.div(n, 8), lax.rem(n, 8)

        @pl.when(pair_row + i < 3)
        def _():
            @pl.when(turn == 0)
            def _():
                waits(qg.at[i], q_recv.at[i])
                acc[...] = jnp.zeros_like(acc)
                carry[...] = jnp.zeros_like(carry)

            attend_two(i, 15 - 2 * turn)

            @pl.when(turn == 7)
            def _():
                part[i] = acc[...].astype(BF16)
                for r in range(4):
                    column = jnp.broadcast_to(carry[r * 128 : r * 128 + 128, :], (128, 128))
                    total_out[i, r] = column.T[0:8, :]
                for copy in part_copies(i):
                    copy.start()

        return 0

    def for_own(n, _):
        w_loop(w_others + 4 * n, w_others + 4 * n + 4)
        newer = here - 1 - 2 * n

        @pl.when(newer >= 1)
        def _():
            attend_two(3, jnp.maximum(newer, 1))

        @pl.when(newer == 0)
        def _():
            attend(3, 0, False)

        return 0

    w_others = w_first_steps
    lax.fori_loop(0, 24, for_others, 0)
    acc[...] = jnp.zeros_like(acc)
    carry[...] = jnp.zeros_like(carry)
    attend(3, here, True)
    lax.fori_loop(0, 8, for_own, 0)
    for p in (2, 1, 0):

        @pl.when(pair_row > p)
        def _():
            waits(part_in.at[p], part_recv.at[p])
            waits(total_in.at[p], total_recv.at[p])
            for r in range(4):
                rows = pl.ds(r * 128, 128)
                after = carry[rows, :]
                acc[rows, :] += jnp.exp2(-after) * part_in[p, rows, :].astype(F32)
                column = jnp.broadcast_to(total_in[p, r, 0:1, :], (128, 128)).T
                carry[rows, :] = after + column[:, 0:1]

    for d in (1, 2, 3):
        source = lax.rem(tp + 4 - d, 4)
        block = owg.at[source, core]
        remote(block, block, ow_send.at[d - 1], ow_recv.at[d - 1], partner).wait_recv()
        remote(block, block, ow_pair_send, ow_pair_recv, partner).start()
    for h in range(2):
        mixed = acc[pl.ds(h * 256, 256), :]
        power = jnp.mean(mixed * mixed, axis=1, keepdims=True)
        lanes = slice(h * 128, h * 128 + 128)
        attg[tp, :, lanes] = (mixed * lax.rsqrt(power + EPS) * gain_ref[0:1, lanes]).astype(BF16)
    for d in (2, 1, 3):
        remote(
            attg.at[tp], attg.at[tp], att_send.at[d - 1], att_recv.at[d - 1], peers[d - 1]
        ).start()
    w_loop(w_others + 32, w_steps - 14)
    waits(owg.at[0:3, 0], ow_pair_recv)
    for d in (1, 2, 3):
        block = resg.at[tp]
        remote(block, block, res_send.at[d - 1], res_recv.at[d - 1], peers[d - 1]).wait_recv()
    for d in (1, 2, 3):
        block = attg.at[tp]
        remote(block, block, att_send.at[d - 1], att_recv.at[d - 1], peers[d - 1]).wait_recv()

    squares = jnp.zeros((256, 1), F32)
    for b in range(4):
        total = resg[b].astype(F32)
        for g in range(4):
            weight = owg[g, b // 2, :, (b % 2) * 512 : (b % 2) * 512 + 512]
            total = total + jnp.dot(attg[g], weight, preferred_element_type=F32)
        hidden = total.astype(BF16)
        hid[b] = hidden
        wide = hidden.astype(F32)
        squares = squares + jnp.sum(wide * wide, axis=1, keepdims=True)
    inverse = lax.rsqrt(squares / 2048.0 + EPS)
    for b in range(4):
        mi[:, b * 512 : b * 512 + 512] = (hid[b].astype(F32) * inverse * mg_ref[b]).astype(BF16)

    w_loop(w_steps - 14, w_steps)
    waits(wg.at[0:4], pair_recv.at[0])
    for b in range(4):
        lifted = jnp.dot(mi[...], wg[(5, 6, 7, 4)[b]], preferred_element_type=F32)
        lifted = jnp.maximum(lifted, 0.0)
        act[b] = (lifted * lifted).astype(BF16)

    def down(owner):
        rows = pl.ds(pl.multiple_of(owner * 512, 512), 512)
        total = jnp.zeros((256, 512), F32)
        for b in range(4):
            total = total + lax.dot_general(
                act[b], wg[b, rows, :], NT, preferred_element_type=F32
            )
        return total

    first, second = pl.ds(0, 128), pl.ds(128, 128)

    def to_peer(n, src, dst, d):
        return remote(src, dst, rs_send.at[n], rs_recv.at[n], peers[d - 1])

    def hand_over():
        return (
            to_peer(0, rs_out.at[0, first], relay_in.at[0], 1),
            to_peer(1, rs_out.at[0, second], relay_in.at[1], 3),
        )

    def direct():
        return (
            to_peer(2, rs_out.at[1, second], rs_in.at[0, second], 1),
            to_peer(3, rs_out.at[2, first], rs_in.at[1, first], 3),
        )

    def combined():
        return (
            to_peer(4, rs_out.at[1, first], rs_in.at[0, first], 1),
            to_peer(5, rs_out.at[2, second], rs_in.at[1, second], 3),
        )

    rs_out[0] = down(lax.rem(tp + 2, 4)).astype(BF16)
    for copy in hand_over():
        copy.start()
    share = down(lax.rem(tp + 1, 4))
    kept[0] = share[0:128]
    rs_out[1, second, :] = share[128:256].astype(BF16)
    direct()[0].start()
    share = down(lax.rem(tp + 3, 4))
    kept[1] = share[128:256]
    rs_out[2, first, :] = share[0:128].astype(BF16)
    direct()[1].start()
    own_part[...] = down(tp) + hid[tp].astype(F32)
    for n in range(2):
        hand_over()[n].wait_recv()
        rs_out[1 + n, (first, second)[n], :] = (kept[n] + relay_in[n].astype(F32)).astype(BF16)
        combined()[n].start()
    for copy in direct() + combined():
        copy.wait_recv()
    out_ref[...] = (own_part[...] + rs_in[0].astype(F32) + rs_in[1].astype(F32)).astype(BF16)

    for n in range(6):
        waits(rs_out.at[0, first], rs_send.at[n])
    for gather in (up_in, down_in):
        for phase in range(2):
            for d in range(2):
                waits(wg.at[0, 0 : 32 * gather.sent(phase, d), :], gather.sem(phase, d))
    waits(wg.at[0:4], pair_send.at[0])
    waits(kvg.at[0], kv_send.at[2])
    for d in range(2):
        waits(kvg.at[0:3], kv_send.at[d])
    waits(kvg.at[0:8], kv_pair_send)
    for i in range(3):

        @pl.when(pair_row > i)
        def _():
            waits(qg.at[i], q_send.at[i])

        @pl.when(pair_row + i < 3)
        def _():
            waits(part.at[i], part_send.at[i])
            waits(total_out.at[i], total_send.at[i])

    waits(owg.at[0:3, 0], ow_pair_send)
    for d in (1, 2, 3):
        waits(res_ref, res_send.at[d - 1])
        waits(owg.at[0, 0], ow_send.at[d - 1])
        waits(attg.at[0], att_send.at[d - 1])


def body(
    residual, queries, key_rows, value_rows, break_shift, head_gain, out_weight, mlp_gain,
    up_weight, down_weight,
):
    vmem = pltpu.VMEM
    dma = pltpu.SemaphoreType.DMA
    return pl.pallas_call(
        kernel,
        out_shape=jax.ShapeDtypeStruct((256, 512), BF16),
        in_specs=[pl.BlockSpec(memory_space=vmem)] * 10,
        out_specs=pl.BlockSpec(memory_space=vmem),
        scratch_shapes=[
            vmem((KV_ROWS, 128), BF16),
            vmem((16, KV_ROWS, 128), BF16),
            vmem((8, 2048, 512), BF16),
            vmem((4, 2, 256, 1024), BF16),
            vmem((4, 256, 512), BF16),
            vmem((4, 256, 256), BF16),
            vmem((4, 512, 128), BF16),
            vmem((3, 512, 128), BF16),
            vmem((3, 4, 8, 128), F32),
            vmem((3, 512, 128), BF16),
            vmem((3, 4, 8, 128), F32),
            vmem((512, 128), F32),
            vmem((512, 1), F32),
            vmem((4, 256, 512), BF16),
            vmem((256, 2048), BF16),
            vmem((4, 256, 512), BF16),
            vmem((3, 256, 512), BF16),
            vmem((2, 256, 512), BF16),
            vmem((2, 128, 512), BF16),
            vmem((2, 128, 512), F32),
            vmem((256, 512), F32),
            dma((KV_PIECES,)),
            dma((2, 2, 2, KV_PIECES)),
            dma((3,)),
            dma,
            dma,
            dma((3,)),
            dma((3,)),
            dma((3,)),
            dma((3,)),
            dma((3,)),
            dma((3,)),
            dma((2, 2, UP_PIECES)),
            dma((2, 4, X_SIZE, UP_PIECES)),
            dma((2, 4, DOWN_PIECES)),
            dma((2, 2, Z_SIZE, DOWN_PIECES)),
            dma((8,)),
            dma((1,)),
            dma((1,)),
            dma((14,)),
            dma((3,)),
            dma((3,)),
            dma,
            dma,
            dma((3,)),
            dma((3,)),
            dma((3,)),
            dma((3,)),
            dma((6,)),
            dma((6,)),
        ],
        compiler_params=pltpu.CompilerParams(
            collective_id=0, has_side_effects=True, vmem_limit_bytes=60 * 1024 * 1024
        ),
        name="layer",
    )(
        residual, queries, key_rows, value_rows, break_shift, head_gain.reshape(1, 256), out_weight,
        mlp_gain.reshape(4, 1, 512), up_weight, down_weight.T,
    )


def solution(mesh):
    in_specs = (
        P("sp", "tp"),
        P("sp", "tp"),
        P("sp", "tp"),
        P("sp", "tp"),
        P("tp", "sp"),
        P("tp"),
        P("tp", None),
        P(),
        P("sp", "tp"),
        P("tp", "sp"),
    )
    return jax.shard_map(
        body, mesh=mesh, in_specs=in_specs, out_specs=P("sp", "tp"), check_vma=False
    )
```

```python
import functools
import math

import jax
import jax.numpy as jnp
from jax import lax
from jax.experimental import pallas as pl
from jax.experimental.pallas import tpu as pltpu
from jax.sharding import PartitionSpec as P

MESH = pl.DeviceIdType.MESH
HEAD_DIM = 128
EPS = 1e-06
LOG2E = 1.4426950408889634
SCALE2 = LOG2E / math.sqrt(HEAD_DIM)
NT = (((1,), (1,)), ((), ()))
F32 = jnp.float32
BF16 = jnp.bfloat16
KV_ROWS = 528
KV_PIECES = 3
KV_PIECE = KV_ROWS // KV_PIECES
UP_PIECES = 2
DOWN_PIECES = 6
X_SIZE, Z_SIZE = 4, 8


def offset_of(k, size):
    return jnp.where(lax.rem(k, 2) == 1, lax.div(k + 1, 2), lax.rem(size - lax.div(k, 2), size))


def last_step(size, direction, even):
    return size // 2 - jnp.where(even == (direction == 0), 0, 1)


def kernel(
    res_ref, q_ref, k_ref, v_ref, shift_ref, gain_ref, ow_ref, mg_ref, up_ref, dn_ref, out_ref,
    kv_ref, kvg, wg, owg, resg, attg, qg, part, total_out, part_in, total_in, acc, carry, hid, mi, act, rs_out, rs_in, relay_in, kept, own_part,
    row_recv, side_recv, kv_send, kv_pair_send, kv_pair_recv, q_send, q_recv,
    part_send, part_recv, total_send, total_recv,
    ua_recv, um_recv, da_recv, dm_recv, gather_send, pair_send, pair_recv,
    local_sem, ow_send, ow_recv, ow_pair_send, ow_pair_recv, res_send, res_recv,
    att_send, att_recv, rs_send, rs_recv,
):
    sp = lax.axis_index("sp")
    tp = lax.axis_index("tp")
    core = lax.rem(sp, 2)
    chip = lax.div(sp, 2)
    x, z = lax.rem(chip, 4), lax.div(chip, 4)
    partner = (sp + 1 - 2 * core, tp)

    def device_at(x, z):
        return 2 * (X_SIZE * z + x) + core

    x_sides = [(device_at(lax.rem(x + d, X_SIZE), z), tp) for d in (1, X_SIZE - 1)]
    z_sides = [(device_at(x, lax.rem(z + d, Z_SIZE)), tp) for d in (1, Z_SIZE - 1)]
    peers = [(sp, lax.rem(tp + d, 4)) for d in (1, 2, 3)]
    z_others = [(device_at(x, lax.rem(z + d, Z_SIZE)), tp) for d in range(1, Z_SIZE)]
    everyone = x_sides + z_others + [partner] + peers

    kv_ref[0:256, :] = k_ref[...]
    kv_ref[272:528, :] = v_ref[...]
    shifts = shift_ref[...].astype(F32)
    shifts = [shifts[:, 0:128], shifts[:, 128:256], jnp.zeros((14, 128), F32)]
    kv_ref[256:272, :] = jnp.concatenate(shifts, axis=0).astype(BF16)

    barrier = pltpu.get_barrier_semaphore()
    for device in everyone:
        pl.semaphore_signal(barrier, inc=1, device_id=device, device_id_type=MESH)
    pl.semaphore_wait(barrier, len(everyone))

    def remote(src, dst, send_sem, recv_sem, device):
        return pltpu.make_async_remote_copy(
            src_ref=src, dst_ref=dst, send_sem=send_sem, recv_sem=recv_sem,
            device_id=device, device_id_type=MESH,
        )

    def waits(ref, sem):
        pltpu.make_async_copy(ref, ref, sem).wait()

    def w_slot(first):
        def slot(origin, piece):
            return wg.at[first + piece, pl.ds(pl.multiple_of(origin * 32, 32), 32), :]

        return slot

    def w_source(page):
        ref, block = (dn_ref, page) if page < 4 else (up_ref, (2, 3, 0, 1)[page - 4])
        return ref.at[:, pl.ds(block * 512, 512)]

    class Gather:
        def __init__(self, number, x_first, pieces, slot, sources, first_recv, main_recv, pair):
            self.x_first, self.pieces, self.slot, self.sources = x_first, pieces, slot, sources
            self.first_recv, self.main_recv, self.pair = first_recv, main_recv, pair
            self.first_size, self.main_size = (X_SIZE, Z_SIZE) if x_first else (Z_SIZE, X_SIZE)
            self.first_to, self.main_to = (x_sides, z_sides) if x_first else (z_sides, x_sides)
            self.sem = lambda phase, d: gather_send.at[number * 4 + phase * 2 + d]

        def origin(self, first, main):
            first_at, main_at = (x, z) if self.x_first else (z, x)
            a = lax.rem(first_at + first, self.first_size)
            b = lax.rem(main_at + main, self.main_size)
            return device_at(a, b) if self.x_first else device_at(b, a)

        def send_first(self, src, dst, d, step, piece):
            return remote(
                src, dst, self.sem(0, d), self.first_recv.at[d, step - 1, piece], self.first_to[d]
            )

        def send_main(self, src, dst, d, step, k, piece):
            return remote(
                src, dst, self.sem(1, d), self.main_recv.at[d, step - 1, k, piece], self.main_to[d]
            )

        def to_partner(self, src, dst):
            remote(src, dst, pair_send.at[self.pair], pair_recv.at[self.pair], partner).start()

        def own_first(self):
            for piece in range(self.pieces):
                src, dst = self.sources[piece], self.slot(sp, piece)
                for d in range(2):
                    self.send_first(src, dst, d, 1, piece).start()

        def own_main(self):
            for piece in range(self.pieces):
                src, dst = self.sources[piece], self.slot(sp, piece)
                for d in range(2):
                    self.send_main(src, dst, d, 1, 0, piece).start()

        def own_near(self):
            for piece in range(self.pieces):
                src, dst = self.sources[piece], self.slot(sp, piece)
                self.to_partner(src, dst)
                keep(src, dst)

        def first_step(self, step, piece):
            for d in range(2):
                last = last_step(self.first_size, d, lax.rem(piece, 2) == 0)
                ahead = self.first_size - step if d == 0 else step
                k = jnp.minimum(2 * step, self.first_size - 1) if d == 0 else 2 * step - 1
                block = self.slot(self.origin(ahead, 0), piece)

                @pl.when(step <= last)
                def _():
                    self.send_first(block, block, d, step, piece).wait_recv()

                @pl.when(step < last)
                def _():
                    self.send_first(block, block, d, step + 1, piece).start()

                @pl.when(step <= last)
                def _():
                    for e in range(2):
                        self.send_main(block, block, e, 1, k, piece).start()
                    self.to_partner(block, block)

        def main_step(self, step, k, piece):
            for d in range(2):
                last = last_step(self.main_size, d, lax.rem(k, 2) == 0)
                ahead = self.main_size - step if d == 0 else step
                block = self.slot(self.origin(offset_of(k, self.first_size), ahead), piece)

                @pl.when(step <= last)
                def _():
                    self.send_main(block, block, d, step, k, piece).wait_recv()

                @pl.when(step < last)
                def _():
                    self.send_main(block, block, d, step + 1, k, piece).start()

                @pl.when(step <= last)
                def _():
                    self.to_partner(block, block)

        def sent(self, phase, d):
            if phase == 0:
                long = [(piece % 2 == 0) == (d == 0) for piece in range(self.pieces)]
                return sum(self.first_size // 2 - (not far) for far in long)
            return self.pieces * self.first_size * (self.main_size - 1) // 2

    locals_ = []

    def keep(src, dst):
        copy = pltpu.make_async_copy(src, dst, local_sem.at[len(locals_)])
        copy.start()
        locals_.append(copy)

    up_in = Gather(
        0, True, UP_PIECES, w_slot(6), [w_source(p) for p in (6, 7)], ua_recv, um_recv, 1
    )
    down_in = Gather(
        1, False, DOWN_PIECES, w_slot(0), [w_source(p) for p in range(6)], da_recv, dm_recv, 0
    )

    row = lax.rem(z, 2)
    here = (row * X_SIZE + x) * 2 + core
    beside = (device_at(x, z + 1 - 2 * row), tp)

    def kv_slot(at_row, at_x, piece, at_core=core):
        start = pl.multiple_of(piece * KV_PIECE, KV_PIECE)
        return kvg.at[(at_row * X_SIZE + at_x) * 2 + at_core, pl.ds(start, KV_PIECE), :]

    def kv_source(piece):
        return kv_ref.at[pl.ds(pl.multiple_of(piece * KV_PIECE, KV_PIECE), KV_PIECE), :]

    def to_row(src, piece):
        return remote(src, kv_slot(row, x, piece), kv_send.at[2], row_recv.at[piece], beside)

    def to_side(src, d, step, at_row, at_x, piece):
        recv = side_recv.at[d, step - 1, at_row, piece]
        return remote(src, kv_slot(at_row, at_x, piece), kv_send.at[d], recv, x_sides[d])

    def to_core(src, at_row, at_x, piece):
        remote(src, kv_slot(at_row, at_x, piece), kv_pair_send, kv_pair_recv, partner).start()

    def send_own(piece, _):
        src = kv_source(piece)
        to_row(src, piece).start()
        for d in range(2):
            to_side(src, d, 1, row, x, piece).start()
        to_core(src, row, x, piece)
        return 0

    lax.fori_loop(0, KV_PIECES, send_own, 0)
    keep(kv_ref, kvg.at[here])
    pair_row = lax.div(z, 2)

    def server_of(p):
        odd = z <= p + 4
        return jnp.where(odd, 2 * p + 1, 2 * p), jnp.where(odd, z - 2 * p - 2, 7 - z)

    def client_at(i):
        return (device_at(x, jnp.where(lax.rem(z, 2) == 1, z + 1 + i, 7 - i)), tp)

    def send_queries(turn):
        for p in range(3):
            at, i = server_of(p)

            @pl.when((pair_row > p) & (i == turn))
            def _():
                for h in range(2):
                    remote(
                        q_ref.at[:, pl.ds(h * 128, 128)], qg.at[turn, pl.ds(h * 256, 256), :],
                        q_send.at[p], q_recv.at[turn], (device_at(x, at), tp),
                    ).start()

    send_queries(0)
    for h in range(2):
        keep(q_ref.at[:, pl.ds(h * 128, 128)], qg.at[3, pl.ds(h * 256, 256), :])

    def from_row(piece, _):
        at_row = 1 - row
        block = kv_slot(at_row, x, piece)
        remote(block, block, kv_send.at[2], row_recv.at[piece], beside).wait_recv()
        for d in range(2):
            to_side(block, d, 1, at_row, x, piece).start()
        to_core(block, at_row, x, piece)
        return 0

    def from_side(at_row, step, piece):
        for d in range(2):
            at_x = lax.rem(x + (X_SIZE - step if d == 0 else step), X_SIZE)
            block = kv_slot(at_row, at_x, piece)
            long = at_row == d

            def arrives():
                recv = side_recv.at[d, step - 1, at_row, piece]
                remote(block, block, kv_send.at[d], recv, x_sides[d]).wait_recv()

            if step == 1:
                arrives()

                @pl.when(long)
                def _():
                    to_side(block, d, 2, at_row, at_x, piece).start()

                to_core(block, at_row, at_x, piece)
            else:

                @pl.when(long)
                def _():
                    arrives()
                    to_core(block, at_row, at_x, piece)

    w_first_steps = DOWN_PIECES * Z_SIZE // 2
    w_steps = w_first_steps + DOWN_PIECES * 16

    up_start = DOWN_PIECES * (X_SIZE // 2 + 1)
    up_every = up_start + UP_PIECES * X_SIZE
    up_end = up_every + 3 * UP_PIECES * (16 - X_SIZE)

    def w_step(n):
        step, piece = lax.div(n, DOWN_PIECES) + 1, lax.rem(n, DOWN_PIECES)

        @pl.when(n < w_first_steps)
        def _():
            down_in.first_step(step, piece)

        @pl.when((step > 1) & (step <= X_SIZE // 2 + 1) & (piece < UP_PIECES))
        def _():
            up_in.first_step(step - 1, piece)

        @pl.when(n >= w_first_steps)
        def _():
            group = lax.div(n - w_first_steps, DOWN_PIECES)
            down_in.main_step(lax.div(group, Z_SIZE) + 1, lax.rem(group, Z_SIZE), piece)

        @pl.when((n >= up_start) & ((n < up_every) | ((lax.rem(n - up_every, 3) == 0) & (n < up_end))))
        def _():
            m = jnp.where(n < up_every, n - up_start, UP_PIECES * X_SIZE + lax.div(n - up_every, 3))
            group = lax.div(m, UP_PIECES)
            up_in.main_step(
                lax.div(group, X_SIZE) + 1, lax.rem(group, X_SIZE), lax.rem(m, UP_PIECES)
            )

    def w_loop(first, last):
        lax.fori_loop(first, last, lambda n, _: (w_step(n), 0)[1], 0)

    def near_side(piece, _):
        from_side(row, 1, piece)
        return 0

    def far_sides(piece, _):
        from_side(1 - row, 1, piece)
        from_side(row, 2, piece)
        return 0

    def last_side(piece, _):
        from_side(1 - row, 2, piece)
        return 0

    lax.fori_loop(0, KV_PIECES, from_row, 0)
    lax.fori_loop(0, KV_PIECES, near_side, 0)
    down_in.own_first()
    up_in.own_main()
    up_in.own_near()
    down_in.own_near()
    lax.fori_loop(0, KV_PIECES, far_sides, 0)
    up_in.own_first()
    down_in.own_main()
    w_loop(0, DOWN_PIECES)
    lax.fori_loop(0, KV_PIECES, last_side, 0)
    half = pl.ds(pl.multiple_of(core * 1024, 1024), 1024)
    for d in (1, 2, 3):
        remote(res_ref, resg.at[tp], res_send.at[d - 1], res_recv.at[d - 1], peers[d - 1]).start()
    for d in (1, 2, 3):
        remote(
            ow_ref.at[:, half], owg.at[tp, core], ow_send.at[d - 1], ow_recv.at[d - 1], peers[d - 1]
        ).start()
    for c in range(2):
        keep(ow_ref.at[:, pl.ds(c * 1024, 1024)], owg.at[tp, c])
    keep(res_ref, resg.at[tp])
    waits(kvg.at[0:8], kv_pair_recv)
    for copy in locals_:
        copy.wait()

    key_at = lax.broadcasted_iota(jnp.int32, (256, 256), 0)
    later_keys = (key_at > lax.broadcasted_iota(jnp.int32, (256, 256), 1)).astype(BF16)

    def broken_of(query, block, visible=None):
        keys = kvg[block, 0:256, :]
        shift = kvg[block, 256:272, :].astype(F32) * LOG2E
        shift = jnp.concatenate([shift[0:1, :], shift[1:2, :]], axis=1)
        t = lax.dot_general(qg[query], keys, NT, preferred_element_type=F32) * SCALE2 + shift
        soft = jnp.maximum(t, jnp.log2(1.0 + jnp.exp2(jnp.minimum(t, 126.0))))
        broken = soft if visible is None else jnp.where(visible, soft, 0.0)
        later = jnp.dot(broken.astype(BF16), later_keys, preferred_element_type=F32)
        return t - soft, later, later[:, 0:1] + broken[:, 0:1]

    def attend(query, block, diagonal):
        visible = None
        if diagonal:
            q_pos = lax.rem(lax.broadcasted_iota(jnp.int32, (512, 256), 0), 256)
            visible = lax.broadcasted_iota(jnp.int32, (512, 256), 1) < q_pos
        picked, later, whole = broken_of(query, block, visible)
        after = carry[...]
        weights = jnp.exp2(picked - (later + after))
        if diagonal:
            weights = jnp.where(visible, weights, 0.0)
        values = kvg[block, 272:528, :]
        acc[...] += jnp.dot(weights.astype(BF16), values, preferred_element_type=F32)
        carry[...] = after + whole

    def attend_two(query, newer):
        picked, later, whole = broken_of(query, newer)
        older_picked, older_later, older_whole = broken_of(query, newer - 1)
        after = carry[...]
        older_after = after + whole
        weights = [
            jnp.exp2(older_picked - (older_later + older_after)).astype(BF16),
            jnp.exp2(picked - (later + after)).astype(BF16),
        ]
        values = [kvg[newer - 1, 272:528, :], kvg[newer, 272:528, :]]
        acc[...] += jnp.dot(
            jnp.concatenate(weights, axis=1),
            jnp.concatenate(values, axis=0),
            preferred_element_type=F32,
        )
        carry[...] = older_after + older_whole

    def part_copies(i):
        return (
            remote(
                part.at[i], part_in.at[pair_row], part_send.at[i], part_recv.at[pair_row], client_at(i)
            ),
            remote(
                total_out.at[i], total_in.at[pair_row], total_send.at[i],
                total_recv.at[pair_row], client_at(i),
            ),
        )

    busy = 14

    def for_others(n, _):
        w_loop(
            DOWN_PIECES + lax.div(n * busy + 23, 24), DOWN_PIECES + lax.div((n + 1) * busy + 23, 24)
        )
        for later in (1, 2):

            @pl.when(n == 6 * later - 4)
            def _():
                send_queries(later)

        i, turn = lax.div(n, 8), lax.rem(n, 8)

        @pl.when(pair_row + i < 3)
        def _():
            @pl.when(turn == 0)
            def _():
                waits(qg.at[i], q_recv.at[i])
                acc[...] = jnp.zeros_like(acc)
                carry[...] = jnp.zeros_like(carry)

            attend_two(i, 15 - 2 * turn)

            @pl.when(turn == 7)
            def _():
                part[i] = acc[...].astype(BF16)
                for r in range(4):
                    column = jnp.broadcast_to(carry[r * 128 : r * 128 + 128, :], (128, 128))
                    total_out[i, r] = column.T[0:8, :]
                for copy in part_copies(i):
                    copy.start()

        return 0

    def for_own(n, _):
        w_loop(w_others + 2 * n, w_others + 2 * n + 2)
        newer = here - 1 - 2 * n

        @pl.when(newer >= 1)
        def _():
            attend_two(3, jnp.maximum(newer, 1))

        @pl.when(newer == 0)
        def _():
            attend(3, 0, False)

        return 0

    w_others = DOWN_PIECES + busy
    lax.fori_loop(0, 24, for_others, 0)
    acc[...] = jnp.zeros_like(acc)
    carry[...] = jnp.zeros_like(carry)
    attend(3, here, True)
    lax.fori_loop(0, 8, for_own, 0)
    for p in (2, 1, 0):

        @pl.when(pair_row > p)
        def _():
            waits(part_in.at[p], part_recv.at[p])
            waits(total_in.at[p], total_recv.at[p])
            for r in range(4):
                rows = pl.ds(r * 128, 128)
                after = carry[rows, :]
                acc[rows, :] += jnp.exp2(-after) * part_in[p, rows, :].astype(F32)
                column = jnp.broadcast_to(total_in[p, r, 0:1, :], (128, 128)).T
                carry[rows, :] = after + column[:, 0:1]

    for d in (1, 2, 3):
        source = lax.rem(tp + 4 - d, 4)
        block = owg.at[source, core]
        remote(block, block, ow_send.at[d - 1], ow_recv.at[d - 1], partner).wait_recv()
        remote(block, block, ow_pair_send, ow_pair_recv, partner).start()
    for h in range(2):
        mixed = acc[pl.ds(h * 256, 256), :]
        power = jnp.mean(mixed * mixed, axis=1, keepdims=True)
        lanes = slice(h * 128, h * 128 + 128)
        attg[tp, :, lanes] = (mixed * lax.rsqrt(power + EPS) * gain_ref[0:1, lanes]).astype(BF16)
    for d in (2, 1, 3):
        remote(
            attg.at[tp], attg.at[tp], att_send.at[d - 1], att_recv.at[d - 1], peers[d - 1]
        ).start()
    w_loop(w_others + 16, 80)
    waits(owg.at[0:3, 0], ow_pair_recv)
    for d in (1, 2, 3):
        block = resg.at[tp]
        remote(block, block, res_send.at[d - 1], res_recv.at[d - 1], peers[d - 1]).wait_recv()
    for d in (1, 2, 3):
        block = attg.at[tp]
        remote(block, block, att_send.at[d - 1], att_recv.at[d - 1], peers[d - 1]).wait_recv()

    squares = jnp.zeros((256, 1), F32)
    for b in range(4):
        total = resg[b].astype(F32)
        for g in range(4):
            weight = owg[g, b // 2, :, (b % 2) * 512 : (b % 2) * 512 + 512]
            total = total + jnp.dot(attg[g], weight, preferred_element_type=F32)
        hidden = total.astype(BF16)
        hid[b] = hidden
        wide = hidden.astype(F32)
        squares = squares + jnp.sum(wide * wide, axis=1, keepdims=True)
    inverse = lax.rsqrt(squares / 2048.0 + EPS)
    for b in range(4):
        mi[:, b * 512 : b * 512 + 512] = (hid[b].astype(F32) * inverse * mg_ref[b]).astype(BF16)

    def up(b):
        lifted = jnp.dot(mi[...], wg[(6, 7, 4, 5)[b]], preferred_element_type=F32)
        lifted = jnp.maximum(lifted, 0.0)
        act[b] = (lifted * lifted).astype(BF16)

    w_loop(80, w_steps)
    waits(wg.at[0:2, 0:1024, :], pair_recv.at[1])
    waits(wg.at[0:6, 0:1024, :], pair_recv.at[0])
    for b in range(4):
        up(b)

    def down(owner):
        rows = pl.ds(pl.multiple_of(owner * 512, 512), 512)
        total = jnp.zeros((256, 512), F32)
        for b in range(4):
            total = total + lax.dot_general(
                act[b], wg[b, rows, :], NT, preferred_element_type=F32
            )
        return total

    first, second = pl.ds(0, 128), pl.ds(128, 128)

    def to_peer(n, src, dst, d):
        return remote(src, dst, rs_send.at[n], rs_recv.at[n], peers[d - 1])

    def hand_over():
        return (
            to_peer(0, rs_out.at[0, first], relay_in.at[0], 1),
            to_peer(1, rs_out.at[0, second], relay_in.at[1], 3),
        )

    def direct():
        return (
            to_peer(2, rs_out.at[1, second], rs_in.at[0, second], 1),
            to_peer(3, rs_out.at[2, first], rs_in.at[1, first], 3),
        )

    def combined():
        return (
            to_peer(4, rs_out.at[1, first], rs_in.at[0, first], 1),
            to_peer(5, rs_out.at[2, second], rs_in.at[1, second], 3),
        )

    rs_out[0] = down(lax.rem(tp + 2, 4)).astype(BF16)
    for copy in hand_over():
        copy.start()
    share = down(lax.rem(tp + 1, 4))
    kept[0] = share[0:128]
    rs_out[1, second, :] = share[128:256].astype(BF16)
    direct()[0].start()
    share = down(lax.rem(tp + 3, 4))
    kept[1] = share[128:256]
    rs_out[2, first, :] = share[0:128].astype(BF16)
    direct()[1].start()
    own_part[...] = down(tp) + hid[tp].astype(F32)
    for n in range(2):
        hand_over()[n].wait_recv()
        rs_out[1 + n, (first, second)[n], :] = (kept[n] + relay_in[n].astype(F32)).astype(BF16)
        combined()[n].start()
    for copy in direct() + combined():
        copy.wait_recv()
    out_ref[...] = (own_part[...] + rs_in[0].astype(F32) + rs_in[1].astype(F32)).astype(BF16)

    for n in range(6):
        waits(rs_out.at[0, first], rs_send.at[n])
    for gather in (up_in, down_in):
        for phase in range(2):
            for d in range(2):
                waits(wg.at[0:2, 0 : 16 * gather.sent(phase, d), :], gather.sem(phase, d))
    waits(wg.at[0:6, 0:1024, :], pair_send.at[0])
    waits(wg.at[0:2, 0:1024, :], pair_send.at[1])
    waits(kvg.at[0], kv_send.at[2])
    for d in range(2):
        waits(kvg.at[0:3], kv_send.at[d])
    waits(kvg.at[0:8], kv_pair_send)
    for i in range(3):

        @pl.when(pair_row > i)
        def _():
            waits(qg.at[i], q_send.at[i])

        @pl.when(pair_row + i < 3)
        def _():
            waits(part.at[i], part_send.at[i])
            waits(total_out.at[i], total_send.at[i])

    waits(owg.at[0:3, 0], ow_pair_send)
    for d in (1, 2, 3):
        waits(resg.at[0], res_send.at[d - 1])
        waits(owg.at[0, 0], ow_send.at[d - 1])
        waits(attg.at[0], att_send.at[d - 1])


def body(
    residual, queries, key_rows, value_rows, break_shift, head_gain, out_weight, mlp_gain,
    up_weight, down_weight,
):
    vmem = pltpu.VMEM
    dma = pltpu.SemaphoreType.DMA
    return pl.pallas_call(
        kernel,
        out_shape=jax.ShapeDtypeStruct((256, 512), BF16),
        in_specs=[
            pl.BlockSpec(memory_space=pl.ANY if n in (0, 6) else vmem) for n in range(10)
        ],
        out_specs=pl.BlockSpec(memory_space=vmem),
        scratch_shapes=[
            vmem((KV_ROWS, 128), BF16),
            vmem((16, KV_ROWS, 128), BF16),
            vmem((8, 2048, 512), BF16),
            vmem((4, 2, 256, 1024), BF16),
            vmem((4, 256, 512), BF16),
            vmem((4, 256, 256), BF16),
            vmem((4, 512, 128), BF16),
            vmem((3, 512, 128), BF16),
            vmem((3, 4, 8, 128), F32),
            vmem((3, 512, 128), BF16),
            vmem((3, 4, 8, 128), F32),
            vmem((512, 128), F32),
            vmem((512, 1), F32),
            vmem((4, 256, 512), BF16),
            vmem((256, 2048), BF16),
            vmem((4, 256, 512), BF16),
            vmem((3, 256, 512), BF16),
            vmem((2, 256, 512), BF16),
            vmem((2, 128, 512), BF16),
            vmem((2, 128, 512), F32),
            vmem((256, 512), F32),
            dma((KV_PIECES,)),
            dma((2, 2, 2, KV_PIECES)),
            dma((3,)),
            dma,
            dma,
            dma((3,)),
            dma((3,)),
            dma((3,)),
            dma((3,)),
            dma((3,)),
            dma((3,)),
            dma((2, 2, UP_PIECES)),
            dma((2, 4, X_SIZE, UP_PIECES)),
            dma((2, 4, DOWN_PIECES)),
            dma((2, 2, Z_SIZE, DOWN_PIECES)),
            dma((8,)),
            dma((2,)),
            dma((2,)),
            dma((14,)),
            dma((3,)),
            dma((3,)),
            dma,
            dma,
            dma((3,)),
            dma((3,)),
            dma((3,)),
            dma((3,)),
            dma((6,)),
            dma((6,)),
        ],
        compiler_params=pltpu.CompilerParams(
            collective_id=0, has_side_effects=True, vmem_limit_bytes=60 * 1024 * 1024
        ),
        name="layer",
    )(
        residual, queries, key_rows, value_rows, break_shift, head_gain.reshape(1, 256), out_weight,
        mlp_gain.reshape(4, 1, 512), up_weight, down_weight.T,
    )


def solution(mesh):
    in_specs = (
        P("sp", "tp"),
        P("sp", "tp"),
        P("sp", "tp"),
        P("sp", "tp"),
        P("tp", "sp"),
        P("tp"),
        P("tp", None),
        P(),
        P("sp", "tp"),
        P("tp", "sp"),
    )
    return jax.shard_map(
        body, mesh=mesh, in_specs=in_specs, out_specs=P("sp", "tp"), check_vma=False
    )
```

```python
import functools
import math

import jax
import jax.numpy as jnp
from jax import lax
from jax.experimental import pallas as pl
from jax.experimental.pallas import tpu as pltpu
from jax.sharding import PartitionSpec as P

MESH = pl.DeviceIdType.MESH
HEAD_DIM = 128
EPS = 1e-06
LOG2E = 1.4426950408889634
SCALE2 = LOG2E / math.sqrt(HEAD_DIM)
NT = (((1,), (1,)), ((), ()))
F32 = jnp.float32
BF16 = jnp.bfloat16
KV_ROWS = 528
KV_PIECES = 3
KV_PIECE = KV_ROWS // KV_PIECES
UP_PIECES = 2
DOWN_PIECES = 6
X_SIZE, Z_SIZE = 4, 8


def offset_of(k, size):
    return jnp.where(lax.rem(k, 2) == 1, lax.div(k + 1, 2), lax.rem(size - lax.div(k, 2), size))


def last_step(size, direction, even):
    return size // 2 - jnp.where(even == (direction == 0), 0, 1)


def kernel(
    res_ref, q_ref, k_ref, v_ref, shift_ref, gain_ref, ow_ref, mg_ref, up_ref, dn_ref, out_ref,
    kv_ref, kvg, wg, owg, resg, attg, qg, part, total_out, part_in, total_in, acc, carry, hid, mi, act, rs_out, rs_in, relay_in, kept, own_part,
    row_recv, side_recv, kv_send, kv_pair_send, kv_pair_recv, q_send, q_recv,
    part_send, part_recv, total_send, total_recv,
    ua_recv, um_recv, da_recv, dm_recv, gather_send, pair_send, pair_recv,
    local_sem, ow_send, ow_recv, ow_pair_send, ow_pair_recv, res_send, res_recv,
    att_send, att_recv, rs_send, rs_recv,
):
    sp = lax.axis_index("sp")
    tp = lax.axis_index("tp")
    core = lax.rem(sp, 2)
    chip = lax.div(sp, 2)
    x, z = lax.rem(chip, 4), lax.div(chip, 4)
    partner = (sp + 1 - 2 * core, tp)

    def device_at(x, z):
        return 2 * (X_SIZE * z + x) + core

    x_sides = [(device_at(lax.rem(x + d, X_SIZE), z), tp) for d in (1, X_SIZE - 1)]
    z_sides = [(device_at(x, lax.rem(z + d, Z_SIZE)), tp) for d in (1, Z_SIZE - 1)]
    peers = [(sp, lax.rem(tp + d, 4)) for d in (1, 2, 3)]
    z_others = [(device_at(x, lax.rem(z + d, Z_SIZE)), tp) for d in range(1, Z_SIZE)]
    everyone = x_sides + z_others + [partner] + peers

    kv_ref[0:256, :] = k_ref[...]
    kv_ref[272:528, :] = v_ref[...]
    shifts = shift_ref[...].astype(F32)
    shifts = [shifts[:, 0:128], shifts[:, 128:256], jnp.zeros((14, 128), F32)]
    kv_ref[256:272, :] = jnp.concatenate(shifts, axis=0).astype(BF16)

    barrier = pltpu.get_barrier_semaphore()
    for device in everyone:
        pl.semaphore_signal(barrier, inc=1, device_id=device, device_id_type=MESH)
    pl.semaphore_wait(barrier, len(everyone))

    def remote(src, dst, send_sem, recv_sem, device):
        return pltpu.make_async_remote_copy(
            src_ref=src, dst_ref=dst, send_sem=send_sem, recv_sem=recv_sem,
            device_id=device, device_id_type=MESH,
        )

    def waits(ref, sem):
        pltpu.make_async_copy(ref, ref, sem).wait()

    def w_slot(first):
        def slot(origin, piece):
            return wg.at[first + piece, pl.ds(pl.multiple_of(origin * 32, 32), 32), :]

        return slot

    def w_source(page):
        ref, block = (dn_ref, page) if page < 4 else (up_ref, (2, 3, 0, 1)[page - 4])
        return ref.at[:, pl.ds(block * 512, 512)]

    class Gather:
        def __init__(self, number, x_first, pieces, slot, sources, first_recv, main_recv, pair):
            self.x_first, self.pieces, self.slot, self.sources = x_first, pieces, slot, sources
            self.first_recv, self.main_recv, self.pair = first_recv, main_recv, pair
            self.first_size, self.main_size = (X_SIZE, Z_SIZE) if x_first else (Z_SIZE, X_SIZE)
            self.first_to, self.main_to = (x_sides, z_sides) if x_first else (z_sides, x_sides)
            self.sem = lambda phase, d: gather_send.at[number * 4 + phase * 2 + d]

        def origin(self, first, main):
            first_at, main_at = (x, z) if self.x_first else (z, x)
            a = lax.rem(first_at + first, self.first_size)
            b = lax.rem(main_at + main, self.main_size)
            return device_at(a, b) if self.x_first else device_at(b, a)

        def send_first(self, src, dst, d, step, piece):
            return remote(
                src, dst, self.sem(0, d), self.first_recv.at[d, step - 1, piece], self.first_to[d]
            )

        def send_main(self, src, dst, d, step, k, piece):
            return remote(
                src, dst, self.sem(1, d), self.main_recv.at[d, step - 1, k, piece], self.main_to[d]
            )

        def to_partner(self, src, dst):
            remote(src, dst, pair_send.at[self.pair], pair_recv.at[self.pair], partner).start()

        def own_first(self):
            for piece in range(self.pieces):
                src, dst = self.sources[piece], self.slot(sp, piece)
                for d in range(2):
                    self.send_first(src, dst, d, 1, piece).start()

        def own_main(self):
            for piece in range(self.pieces):
                src, dst = self.sources[piece], self.slot(sp, piece)
                for d in range(2):
                    self.send_main(src, dst, d, 1, 0, piece).start()

        def own_near(self):
            for piece in range(self.pieces):
                src, dst = self.sources[piece], self.slot(sp, piece)
                self.to_partner(src, dst)
                keep(src, dst)

        def first_step(self, step, piece):
            for d in range(2):
                last = last_step(self.first_size, d, lax.rem(piece, 2) == 0)
                ahead = self.first_size - step if d == 0 else step
                k = jnp.minimum(2 * step, self.first_size - 1) if d == 0 else 2 * step - 1
                block = self.slot(self.origin(ahead, 0), piece)

                @pl.when(step <= last)
                def _():
                    self.send_first(block, block, d, step, piece).wait_recv()

                @pl.when(step < last)
                def _():
                    self.send_first(block, block, d, step + 1, piece).start()

                @pl.when(step <= last)
                def _():
                    for e in range(2):
                        self.send_main(block, block, e, 1, k, piece).start()
                    self.to_partner(block, block)

        def main_step(self, step, k, piece):
            for d in range(2):
                last = last_step(self.main_size, d, lax.rem(k, 2) == 0)
                ahead = self.main_size - step if d == 0 else step
                block = self.slot(self.origin(offset_of(k, self.first_size), ahead), piece)

                @pl.when(step <= last)
                def _():
                    self.send_main(block, block, d, step, k, piece).wait_recv()

                @pl.when(step < last)
                def _():
                    self.send_main(block, block, d, step + 1, k, piece).start()

                @pl.when(step <= last)
                def _():
                    self.to_partner(block, block)

        def sent(self, phase, d):
            if phase == 0:
                long = [(piece % 2 == 0) == (d == 0) for piece in range(self.pieces)]
                return sum(self.first_size // 2 - (not far) for far in long)
            return self.pieces * self.first_size * (self.main_size - 1) // 2

    locals_ = []

    def keep(src, dst):
        copy = pltpu.make_async_copy(src, dst, local_sem.at[len(locals_)])
        copy.start()
        locals_.append(copy)

    up_in = Gather(
        0, True, UP_PIECES, w_slot(6), [w_source(p) for p in (6, 7)], ua_recv, um_recv, 1
    )
    down_in = Gather(
        1, False, DOWN_PIECES, w_slot(0), [w_source(p) for p in range(6)], da_recv, dm_recv, 0
    )

    row = lax.rem(z, 2)
    here = (row * X_SIZE + x) * 2 + core
    beside = (device_at(x, z + 1 - 2 * row), tp)

    def kv_slot(at_row, at_x, piece, at_core=core):
        start = pl.multiple_of(piece * KV_PIECE, KV_PIECE)
        return kvg.at[(at_row * X_SIZE + at_x) * 2 + at_core, pl.ds(start, KV_PIECE), :]

    def kv_source(piece):
        return kv_ref.at[pl.ds(pl.multiple_of(piece * KV_PIECE, KV_PIECE), KV_PIECE), :]

    def to_row(src, piece):
        return remote(src, kv_slot(row, x, piece), kv_send.at[2], row_recv.at[piece], beside)

    def to_side(src, d, step, at_row, at_x, piece):
        recv = side_recv.at[d, step - 1, at_row, piece]
        return remote(src, kv_slot(at_row, at_x, piece), kv_send.at[d], recv, x_sides[d])

    def to_core(src, at_row, at_x, piece):
        remote(src, kv_slot(at_row, at_x, piece), kv_pair_send, kv_pair_recv, partner).start()

    def send_own(piece, _):
        src = kv_source(piece)
        to_row(src, piece).start()
        for d in range(2):
            to_side(src, d, 1, row, x, piece).start()
        to_core(src, row, x, piece)
        return 0

    lax.fori_loop(0, KV_PIECES, send_own, 0)
    keep(kv_ref, kvg.at[here])
    pair_row = lax.div(z, 2)

    def server_of(p):
        odd = z <= p + 4
        return jnp.where(odd, 2 * p + 1, 2 * p), jnp.where(odd, z - 2 * p - 2, 7 - z)

    def client_at(i):
        return (device_at(x, jnp.where(lax.rem(z, 2) == 1, z + 1 + i, 7 - i)), tp)

    def send_queries(turn):
        for p in range(3):
            at, i = server_of(p)

            @pl.when((pair_row > p) & (i == turn))
            def _():
                for h in range(2):
                    remote(
                        q_ref.at[:, pl.ds(h * 128, 128)], qg.at[turn, pl.ds(h * 256, 256), :],
                        q_send.at[p], q_recv.at[turn], (device_at(x, at), tp),
                    ).start()

    send_queries(0)
    for h in range(2):
        keep(q_ref.at[:, pl.ds(h * 128, 128)], qg.at[3, pl.ds(h * 256, 256), :])

    def from_row(piece, _):
        at_row = 1 - row
        block = kv_slot(at_row, x, piece)
        remote(block, block, kv_send.at[2], row_recv.at[piece], beside).wait_recv()
        for d in range(2):
            to_side(block, d, 1, at_row, x, piece).start()
        to_core(block, at_row, x, piece)
        return 0

    def from_side(at_row, step, piece):
        for d in range(2):
            at_x = lax.rem(x + (X_SIZE - step if d == 0 else step), X_SIZE)
            block = kv_slot(at_row, at_x, piece)
            long = at_row == d

            def arrives():
                recv = side_recv.at[d, step - 1, at_row, piece]
                remote(block, block, kv_send.at[d], recv, x_sides[d]).wait_recv()

            if step == 1:
                arrives()

                @pl.when(long)
                def _():
                    to_side(block, d, 2, at_row, at_x, piece).start()

                to_core(block, at_row, at_x, piece)
            else:

                @pl.when(long)
                def _():
                    arrives()
                    to_core(block, at_row, at_x, piece)

    w_first_steps = DOWN_PIECES * Z_SIZE // 2
    w_steps = w_first_steps + DOWN_PIECES * 16

    up_start = DOWN_PIECES * (X_SIZE // 2 + 1)
    up_every = up_start + UP_PIECES * X_SIZE
    up_end = up_every + 3 * UP_PIECES * (16 - X_SIZE)

    def w_step(n):
        step, piece = lax.div(n, DOWN_PIECES) + 1, lax.rem(n, DOWN_PIECES)

        @pl.when(n < w_first_steps)
        def _():
            down_in.first_step(step, piece)

        @pl.when((step > 1) & (step <= X_SIZE // 2 + 1) & (piece < UP_PIECES))
        def _():
            up_in.first_step(step - 1, piece)

        @pl.when(n >= w_first_steps)
        def _():
            group = lax.div(n - w_first_steps, DOWN_PIECES)
            down_in.main_step(lax.div(group, Z_SIZE) + 1, lax.rem(group, Z_SIZE), piece)

        @pl.when((n >= up_start) & ((n < up_every) | ((lax.rem(n - up_every, 3) == 0) & (n < up_end))))
        def _():
            m = jnp.where(n < up_every, n - up_start, UP_PIECES * X_SIZE + lax.div(n - up_every, 3))
            group = lax.div(m, UP_PIECES)
            up_in.main_step(
                lax.div(group, X_SIZE) + 1, lax.rem(group, X_SIZE), lax.rem(m, UP_PIECES)
            )

    def w_loop(first, last):
        lax.fori_loop(first, last, lambda n, _: (w_step(n), 0)[1], 0)

    def near_side(piece, _):
        from_side(row, 1, piece)
        return 0

    def far_sides(piece, _):
        from_side(1 - row, 1, piece)
        from_side(row, 2, piece)
        return 0

    def last_side(piece, _):
        from_side(1 - row, 2, piece)
        return 0

    lax.fori_loop(0, KV_PIECES, from_row, 0)
    lax.fori_loop(0, KV_PIECES, near_side, 0)
    down_in.own_first()
    up_in.own_main()
    up_in.own_near()
    down_in.own_near()
    lax.fori_loop(0, KV_PIECES, far_sides, 0)
    down_in.own_main()
    up_in.own_first()
    w_loop(0, DOWN_PIECES)
    lax.fori_loop(0, KV_PIECES, last_side, 0)
    half = pl.ds(pl.multiple_of(core * 1024, 1024), 1024)
    for d in (1, 2, 3):
        remote(res_ref, resg.at[tp], res_send.at[d - 1], res_recv.at[d - 1], peers[d - 1]).start()
    for d in (1, 2, 3):
        remote(
            ow_ref.at[:, half], owg.at[tp, core], ow_send.at[d - 1], ow_recv.at[d - 1], peers[d - 1]
        ).start()
    for c in range(2):
        keep(ow_ref.at[:, pl.ds(c * 1024, 1024)], owg.at[tp, c])
    keep(res_ref, resg.at[tp])
    waits(kvg.at[0:8], kv_pair_recv)
    for copy in locals_:
        copy.wait()

    key_at = lax.broadcasted_iota(jnp.int32, (256, 256), 0)
    later_keys = (key_at > lax.broadcasted_iota(jnp.int32, (256, 256), 1)).astype(BF16)

    def broken_of(query, block, visible=None):
        keys = kvg[block, 0:256, :]
        shift = kvg[block, 256:272, :].astype(F32) * LOG2E
        shift = jnp.concatenate([shift[0:1, :], shift[1:2, :]], axis=1)
        t = lax.dot_general(qg[query], keys, NT, preferred_element_type=F32) * SCALE2 + shift
        soft = jnp.maximum(t, jnp.log2(1.0 + jnp.exp2(jnp.minimum(t, 126.0))))
        broken = soft if visible is None else jnp.where(visible, soft, 0.0)
        later = jnp.dot(broken.astype(BF16), later_keys, preferred_element_type=F32)
        return t - soft, later, later[:, 0:1] + broken[:, 0:1]

    def attend(query, block, diagonal):
        visible = None
        if diagonal:
            q_pos = lax.rem(lax.broadcasted_iota(jnp.int32, (512, 256), 0), 256)
            visible = lax.broadcasted_iota(jnp.int32, (512, 256), 1) < q_pos
        picked, later, whole = broken_of(query, block, visible)
        after = carry[...]
        weights = jnp.exp2(picked - (later + after))
        if diagonal:
            weights = jnp.where(visible, weights, 0.0)
        values = kvg[block, 272:528, :]
        acc[...] += jnp.dot(weights.astype(BF16), values, preferred_element_type=F32)
        carry[...] = after + whole

    def attend_two(query, newer):
        picked, later, whole = broken_of(query, newer)
        older_picked, older_later, older_whole = broken_of(query, newer - 1)
        after = carry[...]
        older_after = after + whole
        weights = [
            jnp.exp2(older_picked - (older_later + older_after)).astype(BF16),
            jnp.exp2(picked - (later + after)).astype(BF16),
        ]
        values = [kvg[newer - 1, 272:528, :], kvg[newer, 272:528, :]]
        acc[...] += jnp.dot(
            jnp.concatenate(weights, axis=1),
            jnp.concatenate(values, axis=0),
            preferred_element_type=F32,
        )
        carry[...] = older_after + older_whole

    def part_copies(i):
        return (
            remote(
                part.at[i], part_in.at[pair_row], part_send.at[i], part_recv.at[pair_row], client_at(i)
            ),
            remote(
                total_out.at[i], total_in.at[pair_row], total_send.at[i],
                total_recv.at[pair_row], client_at(i),
            ),
        )

    busy = 16

    def for_others(n, _):
        w_loop(
            DOWN_PIECES + lax.div(n * busy + 23, 24), DOWN_PIECES + lax.div((n + 1) * busy + 23, 24)
        )
        for later in (1, 2):

            @pl.when(n == 6 * later - 4)
            def _():
                send_queries(later)

        i, turn = lax.div(n, 8), lax.rem(n, 8)

        @pl.when(pair_row + i < 3)
        def _():
            @pl.when(turn == 0)
            def _():
                waits(qg.at[i], q_recv.at[i])
                acc[...] = jnp.zeros_like(acc)
                carry[...] = jnp.zeros_like(carry)

            attend_two(i, 15 - 2 * turn)

            @pl.when(turn == 7)
            def _():
                part[i] = acc[...].astype(BF16)
                for r in range(4):
                    column = jnp.broadcast_to(carry[r * 128 : r * 128 + 128, :], (128, 128))
                    total_out[i, r] = column.T[0:8, :]
                for copy in part_copies(i):
                    copy.start()

        return 0

    def for_own(n, _):
        w_loop(w_others + 2 * n, w_others + 2 * n + 2)
        newer = here - 1 - 2 * n

        @pl.when(newer >= 1)
        def _():
            attend_two(3, jnp.maximum(newer, 1))

        @pl.when(newer == 0)
        def _():
            attend(3, 0, False)

        return 0

    w_others = DOWN_PIECES + busy
    lax.fori_loop(0, 24, for_others, 0)
    acc[...] = jnp.zeros_like(acc)
    carry[...] = jnp.zeros_like(carry)
    attend(3, here, True)
    lax.fori_loop(0, 8, for_own, 0)
    for p in (2, 1, 0):

        @pl.when(pair_row > p)
        def _():
            waits(part_in.at[p], part_recv.at[p])
            waits(total_in.at[p], total_recv.at[p])
            for r in range(4):
                rows = pl.ds(r * 128, 128)
                after = carry[rows, :]
                acc[rows, :] += jnp.exp2(-after) * part_in[p, rows, :].astype(F32)
                column = jnp.broadcast_to(total_in[p, r, 0:1, :], (128, 128)).T
                carry[rows, :] = after + column[:, 0:1]

    for d in (1, 2, 3):
        source = lax.rem(tp + 4 - d, 4)
        block = owg.at[source, core]
        remote(block, block, ow_send.at[d - 1], ow_recv.at[d - 1], partner).wait_recv()
        remote(block, block, ow_pair_send, ow_pair_recv, partner).start()
    for h in range(2):
        mixed = acc[pl.ds(h * 256, 256), :]
        power = jnp.mean(mixed * mixed, axis=1, keepdims=True)
        lanes = slice(h * 128, h * 128 + 128)
        attg[tp, :, lanes] = (mixed * lax.rsqrt(power + EPS) * gain_ref[0:1, lanes]).astype(BF16)
    for d in (2, 1, 3):
        remote(
            attg.at[tp], attg.at[tp], att_send.at[d - 1], att_recv.at[d - 1], peers[d - 1]
        ).start()
    w_loop(w_others + 16, 80)
    waits(owg.at[0:3, 0], ow_pair_recv)
    for d in (1, 2, 3):
        block = resg.at[tp]
        remote(block, block, res_send.at[d - 1], res_recv.at[d - 1], peers[d - 1]).wait_recv()
    for d in (1, 2, 3):
        block = attg.at[tp]
        remote(block, block, att_send.at[d - 1], att_recv.at[d - 1], peers[d - 1]).wait_recv()

    squares = jnp.zeros((256, 1), F32)
    for b in range(4):
        total = resg[b].astype(F32)
        for g in range(4):
            weight = owg[g, b // 2, :, (b % 2) * 512 : (b % 2) * 512 + 512]
            total = total + jnp.dot(attg[g], weight, preferred_element_type=F32)
        hidden = total.astype(BF16)
        hid[b] = hidden
        wide = hidden.astype(F32)
        squares = squares + jnp.sum(wide * wide, axis=1, keepdims=True)
    inverse = lax.rsqrt(squares / 2048.0 + EPS)
    for b in range(4):
        mi[:, b * 512 : b * 512 + 512] = (hid[b].astype(F32) * inverse * mg_ref[b]).astype(BF16)

    def up(b):
        lifted = jnp.dot(mi[...], wg[(6, 7, 4, 5)[b]], preferred_element_type=F32)
        lifted = jnp.maximum(lifted, 0.0)
        act[b] = (lifted * lifted).astype(BF16)

    w_loop(80, w_steps)
    waits(wg.at[0:2, 0:1024, :], pair_recv.at[1])
    waits(wg.at[0:6, 0:1024, :], pair_recv.at[0])
    for b in range(4):
        up(b)

    def down(owner):
        rows = pl.ds(pl.multiple_of(owner * 512, 512), 512)
        total = jnp.zeros((256, 512), F32)
        for b in range(4):
            total = total + lax.dot_general(
                act[b], wg[b, rows, :], NT, preferred_element_type=F32
            )
        return total

    first, second = pl.ds(0, 128), pl.ds(128, 128)

    def to_peer(n, src, dst, d):
        return remote(src, dst, rs_send.at[n], rs_recv.at[n], peers[d - 1])

    def hand_over():
        return (
            to_peer(0, rs_out.at[0, first], relay_in.at[0], 1),
            to_peer(1, rs_out.at[0, second], relay_in.at[1], 3),
        )

    def direct():
        return (
            to_peer(2, rs_out.at[1, second], rs_in.at[0, second], 1),
            to_peer(3, rs_out.at[2, first], rs_in.at[1, first], 3),
        )

    def combined():
        return (
            to_peer(4, rs_out.at[1, first], rs_in.at[0, first], 1),
            to_peer(5, rs_out.at[2, second], rs_in.at[1, second], 3),
        )

    rs_out[0] = down(lax.rem(tp + 2, 4)).astype(BF16)
    for copy in hand_over():
        copy.start()
    share = down(lax.rem(tp + 1, 4))
    kept[0] = share[0:128]
    rs_out[1, second, :] = share[128:256].astype(BF16)
    direct()[0].start()
    share = down(lax.rem(tp + 3, 4))
    kept[1] = share[128:256]
    rs_out[2, first, :] = share[0:128].astype(BF16)
    direct()[1].start()
    own_part[...] = down(tp) + hid[tp].astype(F32)
    for n in range(2):
        hand_over()[n].wait_recv()
        rs_out[1 + n, (first, second)[n], :] = (kept[n] + relay_in[n].astype(F32)).astype(BF16)
        combined()[n].start()
    for copy in direct() + combined():
        copy.wait_recv()
    out_ref[...] = (own_part[...] + rs_in[0].astype(F32) + rs_in[1].astype(F32)).astype(BF16)

    for n in range(6):
        waits(rs_out.at[0, first], rs_send.at[n])
    for gather in (up_in, down_in):
        for phase in range(2):
            for d in range(2):
                waits(wg.at[0:2, 0 : 16 * gather.sent(phase, d), :], gather.sem(phase, d))
    waits(wg.at[0:6, 0:1024, :], pair_send.at[0])
    waits(wg.at[0:2, 0:1024, :], pair_send.at[1])
    waits(kvg.at[0], kv_send.at[2])
    for d in range(2):
        waits(kvg.at[0:3], kv_send.at[d])
    waits(kvg.at[0:8], kv_pair_send)
    for i in range(3):

        @pl.when(pair_row > i)
        def _():
            waits(qg.at[i], q_send.at[i])

        @pl.when(pair_row + i < 3)
        def _():
            waits(part.at[i], part_send.at[i])
            waits(total_out.at[i], total_send.at[i])

    waits(owg.at[0:3, 0], ow_pair_send)
    for d in (1, 2, 3):
        waits(resg.at[0], res_send.at[d - 1])
        waits(owg.at[0, 0], ow_send.at[d - 1])
        waits(attg.at[0], att_send.at[d - 1])


def body(
    residual, queries, key_rows, value_rows, break_shift, head_gain, out_weight, mlp_gain,
    up_weight, down_weight,
):
    vmem = pltpu.VMEM
    dma = pltpu.SemaphoreType.DMA
    return pl.pallas_call(
        kernel,
        out_shape=jax.ShapeDtypeStruct((256, 512), BF16),
        in_specs=[
            pl.BlockSpec(memory_space=pl.ANY if n in (0, 6) else vmem) for n in range(10)
        ],
        out_specs=pl.BlockSpec(memory_space=vmem),
        scratch_shapes=[
            vmem((KV_ROWS, 128), BF16),
            vmem((16, KV_ROWS, 128), BF16),
            vmem((8, 2048, 512), BF16),
            vmem((4, 2, 256, 1024), BF16),
            vmem((4, 256, 512), BF16),
            vmem((4, 256, 256), BF16),
            vmem((4, 512, 128), BF16),
            vmem((3, 512, 128), BF16),
            vmem((3, 4, 8, 128), F32),
            vmem((3, 512, 128), BF16),
            vmem((3, 4, 8, 128), F32),
            vmem((512, 128), F32),
            vmem((512, 1), F32),
            vmem((4, 256, 512), BF16),
            vmem((256, 2048), BF16),
            vmem((4, 256, 512), BF16),
            vmem((3, 256, 512), BF16),
            vmem((2, 256, 512), BF16),
            vmem((2, 128, 512), BF16),
            vmem((2, 128, 512), F32),
            vmem((256, 512), F32),
            dma((KV_PIECES,)),
            dma((2, 2, 2, KV_PIECES)),
            dma((3,)),
            dma,
            dma,
            dma((3,)),
            dma((3,)),
            dma((3,)),
            dma((3,)),
            dma((3,)),
            dma((3,)),
            dma((2, 2, UP_PIECES)),
            dma((2, 4, X_SIZE, UP_PIECES)),
            dma((2, 4, DOWN_PIECES)),
            dma((2, 2, Z_SIZE, DOWN_PIECES)),
            dma((8,)),
            dma((2,)),
            dma((2,)),
            dma((14,)),
            dma((3,)),
            dma((3,)),
            dma,
            dma,
            dma((3,)),
            dma((3,)),
            dma((3,)),
            dma((3,)),
            dma((6,)),
            dma((6,)),
        ],
        compiler_params=pltpu.CompilerParams(
            collective_id=0, has_side_effects=True, vmem_limit_bytes=60 * 1024 * 1024
        ),
        name="layer",
    )(
        residual, queries, key_rows, value_rows, break_shift, head_gain.reshape(1, 256), out_weight,
        mlp_gain.reshape(4, 1, 512), up_weight, down_weight.T,
    )


def solution(mesh):
    in_specs = (
        P("sp", "tp"),
        P("sp", "tp"),
        P("sp", "tp"),
        P("sp", "tp"),
        P("tp", "sp"),
        P("tp"),
        P("tp", None),
        P(),
        P("sp", "tp"),
        P("tp", "sp"),
    )
    return jax.shard_map(
        body, mesh=mesh, in_specs=in_specs, out_specs=P("sp", "tp"), check_vma=False
    )
```
